32 devices in a mesh: fs: 4 (over z), rep: 4 (over y, x), tp: 2 (over core).
Axes of the slice: x: 2, y: 2, z: 4, core: 2. Of those that a mesh axis runs over, the one named last changes fastest.
Arguments:
- normed: bfloat16 [10240, 2048], P(('fs', 'rep')), may hold values from -150 to 150
- rec_cot: bfloat16 [10240, 2048], P(('fs', 'rep'), 'tp'), may hold values from -1.4823177 to 1.4823177
- conv_out: bfloat16 [10240, 2048], P(('fs', 'rep'), 'tp'), may hold values from -6 to 6
- gate_cot: bfloat16 [10240, 2048], P(('fs', 'rep'), 'tp'), may hold values from -0.05908203 to 0.05908203
- rec_weight: float32 [2048, 2048], P('fs', 'tp'), may hold values from -0.125 to 0.125
- rec_moment: float32 [2048, 2048], P('fs', 'tp'), may hold values from -6 to 6
- rec_right: bfloat16 [2048, 256], P('tp'), may hold values from -1 to 2
- gate_weight: float32 [8, 256, 256], P('tp', 'fs'), may hold values from -0.375 to 0.375
- gate_moment: float32 [8, 256, 256], P('tp', 'fs'), may hold values from -6 to 6
- gate_left: bfloat16 [8, 256, 256], P('tp', 'fs'), may hold values from -1 to 2
- gate_right: bfloat16 [8, 256, 256], P('tp'), may hold values from -1 to 2
Outputs:
- rec_weight_new: float32 [2048, 2048], P('fs', 'tp')
- rec_moment_new: float32 [2048, 2048], P('fs', 'tp')
- rec_step: float32 [2048, 2048], P('fs', 'tp')
- rec_copy: bfloat16 [2048, 2048], P('fs', 'tp')
- gate_weight_new: float32 [8, 256, 256], P('tp', 'fs')
- gate_moment_new: float32 [8, 256, 256], P('tp', 'fs')
- gate_step: float32 [8, 256, 256], P('tp', 'fs')
- gate_copy: bfloat16 [8, 256, 256], P('tp', 'fs')
The draws below stay inside these ranges and needn't reach their ends.
All inputs are finite; a program needn't handle non-finite values.
Results may differ from the reference program's by a relative error of at most 0.001.
Values sent between devices are 32-bit elements; how exact they have to be, the bound alone decides.
A program may use at most 64 MiB of HBM per device.

```python
import jax
import jax.numpy as jnp
from jax import lax

D = 2048
D_RNN = 2048
HEADS = 8
BLK = 256
TOKENS = 10240


def rising_scales(key, column_count):
    position = jnp.arange(column_count, dtype=jnp.float32) / column_count
    jitter = jnp.exp(jax.random.uniform(key, (column_count,), jnp.float32, 0.0, jnp.log(3.0)))
    return jnp.exp(jnp.log(4.0) * position) * jitter


def token_matrix(key, column_count, overall):
    key_list = jax.random.split(key, 2)
    scales = rising_scales(key_list[0], column_count) * overall
    values = jnp.clip(jax.random.normal(key_list[1], (TOKENS, column_count), jnp.float32), -6.0, 6.0)
    return values * scales


def identity_plus(key, count, block_size):
    noise = jnp.clip(jax.random.normal(key, (count, block_size, block_size), jnp.float32), -4.0, 4.0)
    symmetric = (noise + jnp.swapaxes(noise, 1, 2)) * (0.5 / jnp.sqrt(2.0 * block_size))
    result = jnp.eye(block_size, dtype=jnp.float32)[None] + symmetric
    return jnp.clip(result, -1.0, 2.0)


def draw_normed(key, part):
    return token_matrix(jax.random.fold_in(key, 11), D, 1.0).astype(jnp.bfloat16)


def draw_rec_cot(key, part):
    return token_matrix(jax.random.fold_in(key, 12), D_RNN, TOKENS ** (-0.5)).astype(jnp.bfloat16)


def draw_rec_right(key, part):
    blocks = identity_plus(jax.random.fold_in(key, 13), D_RNN // BLK, BLK)
    return blocks.reshape(D_RNN, BLK).astype(jnp.bfloat16)


def draw_gate_left(key, part):
    return identity_plus(jax.random.fold_in(key, 14), HEADS, BLK).astype(jnp.bfloat16)


def draw_gate_right(key, part):
    return identity_plus(jax.random.fold_in(key, 15), HEADS, BLK).astype(jnp.bfloat16)


def steps_of(stream_key, dims, pieces, low, high):
    loudness, own = 1.0, jax.random.fold_in(stream_key, 6)
    for dim, parts in pieces:
        draws = jnp.exp(jax.random.uniform(jax.random.fold_in(own, dim), (parts,), jnp.float32, low / len(pieces), high / len(pieces)))
        loudness = loudness * jnp.repeat(draws, dims[dim] // parts).reshape([-1 if axis == dim else 1 for axis in range(len(dims))])
    return loudness


def scatter_about(own_key, extent, scale, bound, pieces=(), kind=jnp.bfloat16):
    values = scale * jax.random.normal(own_key, extent, jnp.float32)
    if pieces:
        values = values * steps_of(own_key, extent, pieces, -0.22, 0.18)
    return jnp.clip(values, -bound, bound).astype(kind)


def setup_inputs(seed: int = 0) -> dict:
    splits = jax.random.split(jax.random.key(seed), 12)
    return {
        "normed": draw_normed(jax.random.fold_in(splits[11], 71), 0),
        "rec_cot": draw_rec_cot(jax.random.fold_in(splits[11], 71), 0),
        "conv_out": scatter_about(splits[2], (TOKENS, D_RNN), 1.0, 6.0, ((0, 16), (1, 2))),
        "gate_cot": scatter_about(splits[3], (TOKENS, D_RNN), (TOKENS ** -0.5), 0.05908203, ((0, 16), (1, 2))),
        "rec_weight": scatter_about(splits[4], (D, D_RNN), D ** -0.5, 0.125, ((0, 4), (1, 2)), jnp.float32),
        "rec_moment": scatter_about(splits[5], (D, D_RNN), 1.0, 6.0, ((0, 4), (1, 2)), jnp.float32),
        "rec_right": draw_rec_right(jax.random.fold_in(splits[11], 71), 0),
        "gate_weight": scatter_about(splits[7], (HEADS, BLK, BLK), BLK ** -0.5, 0.375, ((0, 2), (1, 4)), jnp.float32),
        "gate_moment": scatter_about(splits[8], (HEADS, BLK, BLK), 1.0, 6.0, ((0, 2), (1, 4)), jnp.float32),
        "gate_left": draw_gate_left(jax.random.fold_in(splits[11], 71), 0),
        "gate_right": draw_gate_right(jax.random.fold_in(splits[11], 71), 0),
    }


BETA = 0.9
LEARN_RATE = 0.02
EPSILON = 1e-06

def precondition_right(gradient, factor):
    row_count = gradient.shape[0]
    block_size = factor.shape[1]
    blocks = factor.shape[0] // block_size
    shaped = gradient.reshape(row_count, blocks, block_size)
    factors = factor.astype(jnp.float32).reshape(blocks, block_size, block_size)
    result = jnp.einsum('rbi,bij->rbj', shaped, factors, precision=lax.Precision.HIGHEST)
    return result.reshape(row_count, blocks * block_size)

def apply_update(weight, moment, precond, gradient):
    new_moment = BETA * moment + precond
    scale = jnp.sqrt(jnp.sum(gradient * gradient)) / jnp.sqrt(jnp.sum(new_moment * new_moment) + EPSILON)
    step_taken = LEARN_RATE * scale * new_moment
    new_weight = weight - step_taken
    return (new_weight, new_moment, step_taken, new_weight.astype(jnp.bfloat16))

def reference(normed, rec_cot, conv_out, gate_cot, rec_weight, rec_moment, rec_right, gate_weight, gate_moment, gate_left, gate_right):
    rec_grad = lax.dot_general(normed, rec_cot, (((0,), (0,)), ((), ())), preferred_element_type=jnp.float32)
    rec_pre = precondition_right(rec_grad, rec_right)
    conv_blocks = conv_out.astype(jnp.float32).reshape(TOKENS, HEADS, BLK)
    cot_blocks = gate_cot.astype(jnp.float32).reshape(TOKENS, HEADS, BLK)
    gate_grad = jnp.einsum('thi,thj->hij', conv_blocks, cot_blocks)
    right_done = jnp.einsum('hij,hjk->hik', gate_grad, gate_right.astype(jnp.float32), precision=lax.Precision.HIGHEST)
    gate_pre = jnp.einsum('hij,hjk->hik', gate_left.astype(jnp.float32), right_done, precision=lax.Precision.HIGHEST)
    rec_new, rec_mom, rec_taken, rec_low = apply_update(rec_weight, rec_moment, rec_pre, rec_grad)
    gate_new, gate_mom, gate_taken, gate_low = apply_update(gate_weight, gate_moment, gate_pre, gate_grad)
    return (rec_new, rec_mom, rec_taken, rec_low, gate_new, gate_mom, gate_taken, gate_low)
```

```python
import functools

import jax
import jax.numpy as jnp
from jax import lax
from jax.experimental import pallas as pl
from jax.experimental.pallas import tpu as pltpu
from jax.sharding import PartitionSpec as P

BETA = 0.9
LEARN_RATE = 0.02
EPSILON = 1e-06
MESH = pl.DeviceIdType.MESH
LANES = 128


def split_dot(value, factor):
    high = value.astype(jnp.bfloat16)
    low = (value - high.astype(jnp.float32)).astype(jnp.bfloat16)
    return jnp.dot(high, factor, preferred_element_type=jnp.float32) + jnp.dot(
        low, factor, preferred_element_type=jnp.float32
    )


def split_dot_left(factor, value):
    high = value.astype(jnp.bfloat16)
    low = (value - high.astype(jnp.float32)).astype(jnp.bfloat16)
    return jnp.dot(factor, high, preferred_element_type=jnp.float32) + jnp.dot(
        factor, low, preferred_element_type=jnp.float32
    )


def token_dot(left, right):
    return lax.dot_general(left, right, (((0,), (0,)), ((), ())), preferred_element_type=jnp.float32)


def folded_squares(value):
    squares = value * value
    rows, width = squares.shape
    total = jnp.sum(squares.reshape(rows // 8, 8, width), axis=0)
    result = total[:, :LANES]
    for start in range(LANES, width, LANES):
        result = result + total[:, start : start + LANES]
    return result


def kernel(
    fs_size, tp_size, halves,
    normed_hbm, rec_cot_hbm, conv_hbm, gate_cot_hbm, rec_moment_hbm, rec_right_hbm, gate_moment_hbm, gate_left_hbm,
    gate_right_hbm,
    rec_new, gate_new, scales,
    normed, rec_cot, conv_out, gate_cot, rec_moment, rec_right, gate_moment, gate_left, gate_right,
    part, first, second, along, helped, grad,
    gate_part, gate_first, gate_second, gate_held, gate_along, gate_grad, gate_pre,
    sums, message, slots,
    in_sem, pair_send, pair_recv, ring_send, ring_recv, help_send, help_recv, cube_send, cube_recv, sum_send, sum_recv,
):
    fs, rep, tp = lax.axis_index("fs"), lax.axis_index("rep"), lax.axis_index("tp")
    bits = (lax.rem(rep, 2), rep // 2)
    partners = (rep + 1 - 2 * bits[0], rep + 2 - 4 * bits[1])
    chunks, rows, width = part.shape[0], part.shape[-2], part.shape[-1]
    half_rows = 8 * rows
    fs_rows = halves * half_rows
    blocks = gate_moment.shape[0]
    masks = [2**i - 1 for i in range(1, fs_size.bit_length())]
    by_head = gate_pre is not None
    last = fs_size - 1
    gate = chunks

    copies = []
    starts = {}

    def load(name, source, target):
        copy = pltpu.make_async_copy(source, target, in_sem.at[len(copies)])
        copies.append(copy)
        starts.setdefault(name, []).append(copy)

    def column(k):
        return slice(k * width, (k + 1) * width)

    def load_half(half):
        for owner in range(fs_size):
            begin = owner * fs_rows + half * half_rows
            span = slice(begin, begin + half_rows)
            load(("normed", half), normed_hbm.at[:, span], normed.at[:, span])

    load(("cot", 0), rec_cot_hbm.at[:, column(0)], rec_cot.at[:, column(0)])
    load_half(0)
    load("gate", conv_hbm, conv_out)
    load("gate", gate_cot_hbm, gate_cot)
    for half in range(1, halves):
        load_half(half)
    for k in range(1, chunks // halves):
        load(("cot", k), rec_cot_hbm.at[:, column(k)], rec_cot.at[:, column(k)])
    load("right", rec_right_hbm, rec_right)
    load("moment", rec_moment_hbm, rec_moment)
    load("factors", gate_right_hbm, gate_right)
    load("factors", gate_left_hbm, gate_left)
    load("gate moment", gate_moment_hbm, gate_moment)
    for copy in copies:
        copy.start()

    def loaded(name):
        for copy in starts.pop(name, ()):
            copy.wait()

    others = [(i, j) for i in range(fs_size) for j in range(tp_size) if i or j]
    direct = len(others) < 16
    if not direct:
        others = [(i, 0) for i in range(1, fs_size)] + [(0, j) for j in range(1, tp_size)]
    peers = [{"fs": lax.rem(fs + i, fs_size), "tp": lax.rem(tp + j, tp_size)} for i, j in others]

    barrier = pltpu.get_barrier_semaphore()
    greeted = peers + [{"rep": p} for p in partners]
    for peer in greeted:
        pl.semaphore_signal(barrier, inc=1, device_id=peer, device_id_type=MESH)
    sums[...] = jnp.zeros_like(sums)

    def remote(source, target, send, recv, peer):
        return pltpu.make_async_remote_copy(
            src_ref=source, dst_ref=target, send_sem=send, recv_sem=recv,
            device_id=peer, device_id_type=MESH,
        )

    def mine(s):
        return bits[s], bits[1 - s]

    def pair(unit, s, index, side, source, target):
        return remote(
            source, target, pair_send.at[unit, s, index], pair_recv.at[unit, s, index], {"rep": partners[side]}
        )

    def first_pair(k, s):
        a, _ = mine(s)
        return pair(k, s, 0, s, part.at[k, s, 1 - a], first.at[k, s])

    def second_pair(k, s):
        a, b = mine(s)
        return pair(k, s, 1, 1 - s, part.at[k, s, a, 1 - b, fs], second.at[k, s])

    def gather_pair(k, s, level):
        a, b = mine(s)
        whole = gate_grad if k == gate else grad.at[k]
        here = whole.at[s, a, b] if level == 0 else whole.at[s, a]
        return pair(k, s, 2 + level, 1 - s if level == 0 else s, here, here)

    def ring(k, s, step):
        a, _ = mine(s)
        peer = lax.rem(fs + step, fs_size)
        return remote(
            part.at[k, s, a, :, peer], along.at[k, s, step - 1],
            ring_send.at[k, s, step - 1], ring_recv.at[k, s, step - 1], {"fs": peer},
        )

    def helper(k, s):
        a, _ = mine(s)
        return remote(
            part.at[k, s, a, :, last - fs], helped.at[k, s], help_send.at[k, s], help_recv.at[k, s],
            {"fs": jnp.where(fs == 0, 1, last - 1)},
        )

    at_end = (fs == 0) | (fs == last)
    beside = (fs == 1) | (fs == last - 1)
    fold_step = jnp.where(fs == 1, last - 1, 2)

    def when(condition, action):
        if condition is None:
            action()
        else:
            pl.when(condition)(action)

    def sends(step):
        skip = []
        if step == last:
            skip.append(fs == 0)
        if step == 1:
            skip.append(fs == last)
        if step == last - 1:
            skip.append(fs == 1)
        if step == 2:
            skip.append(fs == last - 1)
        return jnp.logical_not(functools.reduce(jnp.logical_or, skip)) if skip else None

    def receives(step):
        if step == last:
            return fs != last
        if step == 1:
            return fs != 0
        return None

    def product(unit):
        if unit == gate:
            loaded("gate")

            @pl.loop(0, blocks)
            def _(block):
                columns = pl.ds(pl.multiple_of(block * width, width), width)
                term = token_dot(conv_out[:, columns], gate_cot[:, columns])
                if by_head:
                    each, half = gate_part.shape[3], gate_part.shape[4]
                    head, place = block // each, lax.rem(block, each)
                    gate_part[0, head // 2, lax.rem(head, 2), place] = term[:half]
                    gate_part[1, lax.rem(head, 2), head // 2, place] = term[half:]
                else:
                    gate_part[:, :, :, block] = term.reshape(2, 2, 2, gate_part.shape[4], width)
        else:
            k, half = unit // halves, unit % halves
            loaded(("cot", k))
            loaded(("normed", half))

            @pl.loop(0, fs_size)
            def _(owner):
                start = pl.multiple_of(owner * fs_rows + half * half_rows, half_rows)
                term = token_dot(normed[:, pl.ds(start, half_rows)], rec_cot[:, column(k)])
                part[unit, :, :, :, owner] = term.reshape(2, 2, 2, rows, width)

    def open_rec(k):
        product(k)
        if k == 0:
            pl.semaphore_wait(barrier, len(greeted))
        for s in range(2):
            first_pair(k, s).start()

    def spread(k):
        for s in range(2):
            first_pair(k, s).wait_recv()
            a, _ = mine(s)

            @pl.loop(0, fs_size)
            def _(owner):
                for b in range(2):
                    part[k, s, a, b, owner] += first[k, s, b, owner]

            pl.when(at_end)(lambda s=s: helper(k, s).start())
            for step in range(1, fs_size):
                when(sends(step), lambda s=s, step=step: ring(k, s, step).start())

    def fold(k):
        @pl.when(beside)
        def _():
            for s in range(2):
                helper(k, s).wait_recv()
                a, _ = mine(s)
                part[k, s, a, :, lax.rem(fs + fold_step, fs_size)] += helped[k, s]
                ring(k, s, fold_step).start()

    def collect(k):
        for s in range(2):
            a, _ = mine(s)
            for step in range(1, fs_size):
                def take(s=s, step=step, a=a):
                    ring(k, s, step).wait_recv()
                    part[k, s, a, :, fs] += along[k, s, step - 1]

                when(receives(step), take)
            second_pair(k, s).start()

    def settle(k):
        for s in range(2):
            second_pair(k, s).wait_recv()
            a, b = mine(s)
            grad[k, s, a, b] = part[k, s, a, b, fs] + second[k, s]
            gather_pair(k, s, 0).start()

    def forward(k):
        for s in range(2):
            gather_pair(k, s, 0).wait_recv()
            gather_pair(k, s, 1).start()

    def finish(k):
        for s in range(2):
            gather_pair(k, s, 1).wait_recv()
        loaded("right")
        loaded("moment")
        columns = column(k // halves)
        here = slice(k % halves * half_rows, (k % halves + 1) * half_rows)
        gradient = grad[k].reshape(half_rows, width)
        moment = BETA * rec_moment[here, columns] + split_dot(gradient, rec_right[columns, :])
        rec_new[here, columns] = moment
        sums[0] += folded_squares(gradient)
        sums[1] += folded_squares(moment)

    def gate_pair(s, index):
        a, b = mine(s)
        if index == 0:
            return pair(gate, s, 0, s, gate_part.at[s, 1 - a], gate_first.at[s])
        return pair(gate, s, 1, 1 - s, gate_part.at[s, a, 1 - b], gate_second.at[s])

    def cube(s, step):
        mask = masks[step] if s == 0 else masks[-1 - step]
        return remote(
            gate_held.at[s, step], gate_along.at[s, step], cube_send.at[s, step], cube_recv.at[s, step],
            {"fs": fs ^ mask},
        )

    def pre_pair(level):
        here = gate_pre.at[bits[0], bits[1]] if level == 0 else gate_pre.at[bits[0]]
        return pair(gate, 0, 2 + level, 1 - level, here, here)

    def open_gate():
        product(gate)
        for s in range(2):
            gate_pair(s, 0).start()

    def gate_add_first():
        for s in range(2):
            gate_pair(s, 0).wait_recv()
            a, _ = mine(s)
            gate_part[s, a] += gate_first[s]
            gate_pair(s, 1).start()

    def gate_add_second():
        for s in range(2):
            gate_pair(s, 1).wait_recv()
            a, b = mine(s)
            gate_held[s, 0] = gate_part[s, a, b] + gate_second[s]
            cube(s, 0).start()

    def gate_cube(step):
        for s in range(2):
            cube(s, step).wait_recv()
            total = gate_held[s, step] + gate_along[s, step]
            if step + 1 < len(masks):
                gate_held[s, step + 1] = total
                cube(s, step + 1).start()
            elif by_head:
                half = gate_part.shape[4]
                gate_grad[:, s * half : (s + 1) * half] = total
            else:
                a, b = mine(s)
                gate_grad[s, a, b] = total
                gather_pair(gate, s, 0).start()
        if by_head and step + 1 == len(masks):
            loaded("factors")
            each, own = gate_part.shape[3], gate_left.shape[1]
            for place in range(each):
                block = (2 * bits[0] + bits[1]) * each + place
                gradient = gate_grad[place]
                right_done = split_dot(gradient, gate_right[block])
                gate_pre[bits[0], bits[1], place, 0:own] = split_dot_left(gate_left[block], right_done)
                gate_pre[bits[0], bits[1], place, own:] = jnp.concatenate(
                    [folded_squares(gradient), jnp.zeros((8, width - LANES), jnp.float32)], axis=1
                )
            pre_pair(0).start()

    def gate_forward():
        if by_head:
            pre_pair(0).wait_recv()
            pre_pair(1).start()
        else:
            forward(gate)

    def gate_finish():
        loaded("gate moment")
        if by_head:
            pre_pair(1).wait_recv()
            each, own = gate_part.shape[3], gate_left.shape[1]
            for block in range(blocks):
                head, place = block // each, block % each
                moment = BETA * gate_moment[block] + gate_pre[head // 2, head % 2, place, 0:own]
                gate_new[block] = moment
                sums[2] += gate_pre[head // 2, head % 2, place, own:, 0:LANES] * (1.0 / fs_size)
                sums[3] += folded_squares(moment)
        else:
            for s in range(2):
                gather_pair(gate, s, 1).wait_recv()
            loaded("factors")

            @pl.loop(0, blocks)
            def _(block):
                gradient = gate_grad[:, :, :, block].reshape(width, width)
                right_done = split_dot(gradient, gate_right[block])
                moment = BETA * gate_moment[block] + split_dot_left(gate_left[block], right_done)
                gate_new[block] = moment
                sums[2] += folded_squares(gradient) * (1.0 / fs_size)
                sums[3] += folded_squares(moment)

    def rec_stages(k):
        return [functools.partial(f, k) for f in (open_rec, spread, fold, collect, settle, forward, finish)]

    gate_stages = [open_gate, gate_add_first, gate_add_second]
    gate_stages += [functools.partial(gate_cube, step) for step in range(len(masks))]
    gate_stages += [gate_forward, gate_finish]
    units = [rec_stages(k) for k in range(chunks)]
    units.insert(1, gate_stages)

    for tick in range(len(units) + max(len(unit) for unit in units)):
        for place in range(min(tick, len(units) - 1), -1, -1):
            stage = tick - place
            if stage < len(units[place]):
                units[place][stage]()

    for i in range(4):
        message[i : i + 1] = jnp.sum(sums[i], axis=0, keepdims=True)
    message[4:8] = jnp.zeros((4, LANES), jnp.float32)

    def exchange(begin, end):
        trades = [
            remote(message, slots.at[i], sum_send.at[i], sum_recv.at[i], peers[i]) for i in range(begin, end)
        ]
        for trade in trades:
            trade.start()
        for trade in trades:
            trade.wait()
        total = message[...]
        for i in range(begin, end):
            total = total + slots[i]
        return total

    if direct:
        total = exchange(0, len(peers))
    else:
        message[...] = exchange(0, fs_size - 1)
        total = exchange(fs_size - 1, len(peers))
    squares = [jnp.sum(total[i : i + 1], keepdims=True) for i in range(4)]
    rec_scale = jnp.sqrt(squares[0]) / jnp.sqrt(squares[1] + EPSILON)
    gate_scale = jnp.sqrt(squares[2]) / jnp.sqrt(squares[3] + EPSILON)
    scales[0] = jnp.broadcast_to(rec_scale, (8, LANES))
    scales[1] = jnp.broadcast_to(gate_scale, (8, LANES))

    for s in range(2):
        for k in range(chunks):
            first_pair(k, s).wait_send()
            second_pair(k, s).wait_send()
            pl.when(at_end)(lambda k=k, s=s: helper(k, s).wait_send())
            pl.when(beside)(lambda k=k, s=s: ring(k, s, fold_step).wait_send())
            for step in range(1, fs_size):
                when(sends(step), lambda k=k, s=s, step=step: ring(k, s, step).wait_send())
            for level in range(2):
                gather_pair(k, s, level).wait_send()
        for index in range(2):
            gate_pair(s, index).wait_send()
            if not by_head:
                gather_pair(gate, s, index).wait_send()
        for step in range(len(masks)):
            cube(s, step).wait_send()
    if by_head:
        for level in range(2):
            pre_pair(level).wait_send()


def shards(fs_size, rep_size, tp_size, normed, rec_cot, conv_out, gate_cot, rec_weight, rec_moment,
           rec_right, gate_weight, gate_moment, gate_left, gate_right):
    assert rep_size == 4 and fs_size & (fs_size - 1) == 0 and fs_size >= 4
    f32 = jnp.float32
    fs_rows, columns = rec_weight.shape
    width = rec_right.shape[1]
    blocks, gate_rows = gate_weight.shape[:2]
    halves = 2 if fs_rows % 256 == 0 else 1
    chunks = columns // width * halves
    rows = fs_rows // (8 * halves)
    others = fs_size - 1
    cubes = fs_size.bit_length() - 1
    peers = fs_size * tp_size - 1 if fs_size * tp_size <= 16 else fs_size + tp_size - 2
    loads = columns // width + halves * fs_size + 7
    operands = (normed, rec_cot, conv_out, gate_cot, rec_moment, rec_right, gate_moment, gate_left, gate_right)
    vmem = pl.BlockSpec(memory_space=pltpu.VMEM)
    if blocks % 4 == 0:
        piece = (blocks // 4, width // 2, width)
        gate_grad = pltpu.VMEM((blocks // 4, width, width), f32)
        gate_pre = pltpu.VMEM((2, 2, blocks // 4, gate_rows + 8, width), f32)
    else:
        piece = (blocks, width // 8, width)
        gate_grad = pltpu.VMEM((2, 2, 2, *piece), f32)
        gate_pre = None
    rec_new, gate_new, scales = pl.pallas_call(
        functools.partial(kernel, fs_size, tp_size, halves),
        out_shape=(
            jax.ShapeDtypeStruct(rec_weight.shape, f32),
            jax.ShapeDtypeStruct(gate_weight.shape, f32),
            jax.ShapeDtypeStruct((2, 8, LANES), f32),
        ),
        in_specs=[pl.BlockSpec(memory_space=pltpu.HBM)] * len(operands),
        out_specs=(vmem,) * 3,
        scratch_shapes=[
            *(pltpu.VMEM(x.shape, x.dtype) for x in operands),
            pltpu.VMEM((chunks, 2, 2, 2, fs_size, rows, width), f32),
            pltpu.VMEM((chunks, 2, 2, fs_size, rows, width), f32),
            pltpu.VMEM((chunks, 2, rows, width), f32),
            pltpu.VMEM((chunks, 2, others, 2, rows, width), f32),
            pltpu.VMEM((chunks, 2, 2, rows, width), f32),
            pltpu.VMEM((chunks, 2, 2, 2, rows, width), f32),
            pltpu.VMEM((2, 2, 2, *piece), f32),
            pltpu.VMEM((2, 2, *piece), f32),
            pltpu.VMEM((2, *piece), f32),
            pltpu.VMEM((2, cubes, *piece), f32),
            pltpu.VMEM((2, cubes, *piece), f32),
            gate_grad,
            gate_pre,
            pltpu.VMEM((4, 8, LANES), f32),
            pltpu.VMEM((8, LANES), f32),
            pltpu.VMEM((peers, 8, LANES), f32),
            pltpu.SemaphoreType.DMA((loads,)),
            pltpu.SemaphoreType.DMA((chunks + 1, 2, 4)),
            pltpu.SemaphoreType.DMA((chunks + 1, 2, 4)),
            pltpu.SemaphoreType.DMA((chunks, 2, others)),
            pltpu.SemaphoreType.DMA((chunks, 2, others)),
            pltpu.SemaphoreType.DMA((chunks, 2)),
            pltpu.SemaphoreType.DMA((chunks, 2)),
            pltpu.SemaphoreType.DMA((2, cubes)),
            pltpu.SemaphoreType.DMA((2, cubes)),
            pltpu.SemaphoreType.DMA((peers,)),
            pltpu.SemaphoreType.DMA((peers,)),
        ],
        compiler_params=pltpu.CompilerParams(
            collective_id=0, has_side_effects=True, vmem_limit_bytes=62 * 1024 * 1024
        ),
    )(*operands)

    def update(weight, moment_new, scale):
        taken = LEARN_RATE * scale * moment_new
        new = weight - taken
        return new, moment_new, taken, new.astype(jnp.bfloat16)

    return update(rec_weight, rec_new, scales[0, 0, 0]) + update(gate_weight, gate_new, scales[1, 0, 0])


def solution(mesh):
    in_specs = (
        P(("fs", "rep"), None),
        P(("fs", "rep"), "tp"),
        P(("fs", "rep"), "tp"),
        P(("fs", "rep"), "tp"),
        P("fs", "tp"),
        P("fs", "tp"),
        P("tp", None),
        P("tp", "fs", None),
        P("tp", "fs", None),
        P("tp", "fs", None),
        P("tp", None, None),
    )
    out_specs = (P("fs", "tp"),) * 4 + (P("tp", "fs", None),) * 4
    body = functools.partial(shards, mesh.shape["fs"], mesh.shape["rep"], mesh.shape["tp"])
    return jax.shard_map(body, mesh=mesh, in_specs=in_specs, out_specs=out_specs, check_vma=False)
```

```python
import functools
import itertools
import math

import jax
import jax.numpy as jnp
from jax import lax
from jax.experimental import pallas as pl
from jax.experimental.pallas import tpu as pltpu
from jax.sharding import PartitionSpec as P

BETA = 0.9
LEARN_RATE = 0.02
EPSILON = 1e-06
MESH = pl.DeviceIdType.MESH
LANES = 128
PARTS = 4
GATE_PLACE = 7
REC_AT = (0, 1, 2, 3, 4, 5, 6)
GATE_AT = (0, 1, 2, 3, 4, 5, 6, 7)


def split_dot(value, factor):
    high = value.astype(jnp.bfloat16)
    low = (value - high.astype(jnp.float32)).astype(jnp.bfloat16)
    return jnp.dot(high, factor, preferred_element_type=jnp.float32) + jnp.dot(
        low, factor, preferred_element_type=jnp.float32
    )


def split_dot_left(factor, value):
    high = value.astype(jnp.bfloat16)
    low = (value - high.astype(jnp.float32)).astype(jnp.bfloat16)
    return jnp.dot(factor, high, preferred_element_type=jnp.float32) + jnp.dot(
        factor, low, preferred_element_type=jnp.float32
    )


def token_dot(left, right):
    return lax.dot_general(left, right, (((0,), (0,)), ((), ())), preferred_element_type=jnp.float32)


def folded_squares(value):
    squares = value * value
    rows, width = squares.shape
    total = jnp.sum(squares.reshape(rows // 8, 8, width), axis=0)
    result = total[:, :LANES]
    for start in range(LANES, width, LANES):
        result = result + total[:, start : start + LANES]
    return result


def plan(fs_rows, column_count):
    units = []
    for column in range(column_count):
        sizes = [256] * (fs_rows // 256) or [fs_rows]
        if len(sizes) > 1 and column == 0:
            sizes = [128, 128] + sizes[1:]
        if len(sizes) > 1 and column == column_count - 1:
            sizes = sizes[:-1] + [128, 128]
        start = 0
        for size in sizes:
            units.append((column, start, size, (column * fs_rows + start) // 8))
            start += size
    return units


def kernel(
    fs_size, tp_size, units,
    normed_hbm, rec_cot_hbm, conv_hbm, gate_cot_hbm, rec_moment_hbm, rec_right_hbm, gate_moment_hbm, gate_left_hbm,
    gate_right_hbm,
    rec_new, gate_new, scales,
    normed, rec_cot, conv_out, gate_cot, rec_moment, rec_right, gate_moment, gate_left, gate_right,
    part, first, second, along, helped, grad,
    gate_part, gate_first, gate_second, gate_held, gate_along, gate_helped, gate_grad, gate_pre,
    sums, message, slots,
    in_sem, rec_send, pair_recv, ring_recv, help_recv,
    gate_send, gate_recv, spread_recv, pre_send, pre_recv, cube_send, cube_recv, sum_send, sum_recv,
):
    fs, rep, tp = lax.axis_index("fs"), lax.axis_index("rep"), lax.axis_index("tp")
    bits = (lax.rem(rep, 2), rep // 2)
    partners = (rep + 1 - 2 * bits[0], rep + 2 - 4 * bits[1])
    width = part.shape[-1]
    fs_rows = rec_moment.shape[0]
    blocks = gate_moment.shape[0]
    masks = [2**i - 1 for i in range(1, fs_size.bit_length())]
    by_head = gate_pre is not None
    last = fs_size - 1
    gate = len(units)

    copies = []
    waits = {}

    def load(name, source, target, sem=None):
        sem = in_sem.at[len(waits)] if sem is None else sem
        copies.append(pltpu.make_async_copy(source, target, sem))
        waits.setdefault(name, (target, sem))
        return sem

    def column_of(k):
        return slice(units[k][0] * width, (units[k][0] + 1) * width)

    def fetch_columns(column):
        span = slice(column * width, (column + 1) * width)
        load(("cot", column), rec_cot_hbm.at[:, span], rec_cot.at[:, span])

    fetch_columns(0)
    for column, start, size, _ in units:
        if column == 0:
            sem = None
            for owner in range(fs_size):
                span = slice(owner * fs_rows + start, owner * fs_rows + start + size)
                sem = load(("normed", start), normed_hbm.at[:, span], normed.at[:, span], sem)
            waits["normed", start] = (normed.at[:, 0 : fs_size * size], sem)
            if start == 0:
                load("conv", conv_hbm, conv_out)
                load("gate", gate_cot_hbm, gate_cot)
    for column in range(1, units[-1][0] + 1):
        fetch_columns(column)
    load("right", rec_right_hbm, rec_right)
    load("moment", rec_moment_hbm, rec_moment)
    load("gate right", gate_right_hbm, gate_right)
    load("gate left", gate_left_hbm, gate_left)
    load("gate moment", gate_moment_hbm, gate_moment)
    for copy in copies:
        copy.start()

    def loaded(*names):
        for name in names:
            if name in waits:
                whole, sem = waits.pop(name)
                pltpu.make_async_copy(whole, whole, sem).wait()

    sizes = {"fs": fs_size, "rep": 4, "tp": tp_size}
    places = {"fs": fs, "rep": rep, "tp": tp}
    direct = math.prod(sizes.values()) <= 32
    groups = [tuple(sizes)] if direct else [(axis,) for axis in ("rep", "fs", "tp")]
    counts = [math.prod(sizes[axis] for axis in axes) for axes in groups]

    def members(axes):
        return [
            {axis: lax.rem(places[axis] + move, sizes[axis]) for axis, move in zip(axes, moves)}
            for moves in itertools.product(*(range(sizes[axis]) for axis in axes))
            if any(moves)
        ]

    barrier = pltpu.get_barrier_semaphore()
    greeted = [peer for axes in groups for peer in members(axes)]
    for peer in greeted:
        pl.semaphore_signal(barrier, inc=1, device_id=peer, device_id_type=MESH)
    sums[...] = jnp.zeros_like(sums)

    def remote(source, target, send, recv, peer):
        return pltpu.make_async_remote_copy(
            src_ref=source, dst_ref=target, send_sem=send, recv_sem=recv,
            device_id=peer, device_id_type=MESH,
        )

    def arrived(whole, recv):
        remote(whole, whole, rec_send.at[0], recv, {"rep": partners[0]}).wait_recv()

    def sent(whole, send):
        remote(whole, whole, send, pair_recv.at[0, 0], {"rep": partners[0]}).wait_send()

    def mine(s):
        return bits[s], bits[1 - s]

    def rows_of(k):
        return slice(units[k][3], units[k][3] + units[k][2] // 8)

    def first_pair(k, s):
        a, _ = mine(s)
        here = rows_of(k)
        return remote(
            part.at[s, 1 - a, :, :, here], first.at[s, :, :, here], rec_send.at[0], pair_recv.at[k, 0],
            {"rep": partners[s]},
        )

    def second_pair(k, s):
        a, b = mine(s)
        here = rows_of(k)
        return remote(
            part.at[s, a, 1 - b, fs, here], second.at[s, here], rec_send.at[2], pair_recv.at[k, 1],
            {"rep": partners[1 - s]},
        )

    def gather_pair(k, s, level):
        a, b = mine(s)
        if level == 0:
            here = grad.at[s, a, b, rows_of(k)]
        else:
            here = grad.at[s, a, :, rows_of(k)]
        return remote(
            here, here, rec_send.at[2], pair_recv.at[k, 2 + level], {"rep": partners[1 - s if level == 0 else s]}
        )

    def chunk(k, s, owner):
        a, b = mine(s)
        return gate_part.at[s, a, b, owner] if k == gate else part.at[s, a, :, owner, rows_of(k)]

    def ring_slot(k, s, step):
        return gate_along.at[s, step - 1] if k == gate else along.at[s, step - 1, :, rows_of(k)]

    def help_slot(k, s):
        return gate_helped.at[s] if k == gate else helped.at[s, :, rows_of(k)]

    def ring_sem(k):
        return gate_send.at[2] if k == gate else rec_send.at[1]

    def ring(k, s, step):
        peer = lax.rem(fs + step, fs_size)
        return remote(chunk(k, s, peer), ring_slot(k, s, step), ring_sem(k), ring_recv.at[k], {"fs": peer})

    def helper(k, s):
        return remote(
            chunk(k, s, last - fs), help_slot(k, s), ring_sem(k), help_recv.at[k],
            {"fs": jnp.where(fs == 0, 1, last - 1)},
        )

    at_end = (fs == 0) | (fs == last)
    beside = (fs == 1) | (fs == last - 1)
    fold_step = jnp.where(fs == 1, last - 1, 2)

    def when(condition, action):
        if condition is None:
            action()
        else:
            pl.when(condition)(action)

    def sends(step):
        skip = []
        if step == last:
            skip.append(fs == 0)
        if step == 1:
            skip.append(fs == last)
        if step == last - 1:
            skip.append(fs == 1)
        if step == 2:
            skip.append(fs == last - 1)
        return jnp.logical_not(functools.reduce(jnp.logical_or, skip)) if skip else None

    def receives(step):
        if step == last:
            return fs != last
        if step == 1:
            return fs != 0
        return None

    def ring_open(k, s):
        pl.when(at_end)(lambda: helper(k, s).start())
        for step in range(1, fs_size):
            when(sends(step), lambda step=step: ring(k, s, step).start())

    def fold(k):
        @pl.when(beside)
        def _():
            arrived(gate_helped if k == gate else helped.at[:, :, rows_of(k)], help_recv.at[k])
            for s in range(2):
                whole = chunk(k, s, lax.rem(fs + fold_step, fs_size))
                whole[...] += help_slot(k, s)[...]
                ring(k, s, fold_step).start()

    def ring_close(k):
        def slots_of(count):
            return gate_along.at[:, 0:count] if k == gate else along.at[:, 0:count, :, rows_of(k)]

        pl.when(at_end)(lambda: arrived(slots_of(last - 1), ring_recv.at[k]))
        pl.when(jnp.logical_not(at_end))(lambda: arrived(slots_of(last), ring_recv.at[k]))
        for s in range(2):
            own = chunk(k, s, fs)
            for step in range(1, fs_size):
                def take(own=own, s=s, step=step):
                    own[...] += ring_slot(k, s, step)[...]

                when(receives(step), take)

    def product(k):
        column, start, size, _ = units[k]
        loaded(("cot", column))
        loaded(("normed", start))

        @pl.loop(0, fs_size)
        def _(owner):
            begin = pl.multiple_of(owner * fs_rows + start, 128)
            term = token_dot(normed[:, pl.ds(begin, size)], rec_cot[:, column_of(k)])
            part[:, :, :, owner, rows_of(k)] = term.reshape(2, 2, 2, size // 8, width)

    def open_rec(k):
        product(k)
        if k == 0:
            pl.semaphore_wait(barrier, len(greeted))
        for s in range(2):
            first_pair(k, s).start()

    def spread(k):
        arrived(first.at[:, :, :, rows_of(k)], pair_recv.at[k, 0])
        for s in range(2):
            a, _ = mine(s)

            @pl.loop(0, fs_size)
            def _(owner):
                for b in range(2):
                    part[s, a, b, owner, rows_of(k)] += first[s, b, owner, rows_of(k)]

            ring_open(k, s)

    def collect(k):
        ring_close(k)
        for s in range(2):
            second_pair(k, s).start()

    def settle(k):
        loaded("right", "moment")
        arrived(second.at[:, rows_of(k)], pair_recv.at[k, 1])
        _, start, size, _ = units[k]
        rows = size // 8
        gradients, moments = [], []
        for s in range(2):
            a, b = mine(s)
            gradients.append(part[s, a, b, fs, rows_of(k)] + second[s, rows_of(k)])
            begin = pl.multiple_of(start + (4 * s + 2 * a + b) * rows, 8)
            moments.append(rec_moment[pl.ds(begin, rows), column_of(k)])
        gradient = jnp.concatenate(gradients, axis=0)
        moment = BETA * jnp.concatenate(moments, axis=0) + split_dot(gradient, rec_right[column_of(k), :])
        for s in range(2):
            a, b = mine(s)
            grad[s, a, b, rows_of(k)] = moment[s * rows : (s + 1) * rows]
            gather_pair(k, s, 0).start()
        sums[0] += folded_squares(gradient)
        sums[1] += folded_squares(moment)

    def forward(k):
        arrived(grad.at[0, :, 0, rows_of(k)], pair_recv.at[k, 2])
        for s in range(2):
            gather_pair(k, s, 1).start()

    def finish(k):
        arrived(grad.at[0, :, :, rows_of(k)], pair_recv.at[k, 3])
        _, start, size, _ = units[k]
        rec_new[start : start + size, column_of(k)] = grad[:, :, :, rows_of(k)].reshape(size, width)

    def gate_pair(s, index):
        a, b = mine(s)
        source, target = (gate_part.at[s, 1 - a], gate_first) if index == 0 else (gate_part.at[s, a, 1 - b], gate_second)
        return remote(
            source, target.at[s], gate_send.at[index], gate_recv.at[index],
            {"rep": partners[s if index == 0 else 1 - s]},
        )

    def open_gate():
        loaded("conv", "gate")

        @pl.loop(0, blocks)
        def _(block):
            columns = pl.ds(pl.multiple_of(block * width, width), width)
            term = token_dot(conv_out[:, columns], gate_cot[:, columns])
            if by_head:
                each, thin = gate_part.shape[4], gate_part.shape[5]
                head, place = block // each, lax.rem(block, each)
                halves = term.reshape(2, fs_size, thin, width)
                gate_part[0, head // 2, lax.rem(head, 2), :, place] = halves[0]
                gate_part[1, lax.rem(head, 2), head // 2, :, place] = halves[1]
            else:
                gate_part[:, :, :, block] = term.reshape(2, 2, 2, gate_part.shape[4], width)

        for s in range(2):
            gate_pair(s, 0).start()

    def gate_add_first():
        arrived(gate_first, gate_recv.at[0])
        for s in range(2):
            a, _ = mine(s)
            gate_part[s, a] += gate_first[s]
            gate_pair(s, 1).start()

    def gate_total(s):
        if s == 0:
            arrived(gate_second, gate_recv.at[1])
        a, b = mine(s)
        return gate_part[s, a, b] + gate_second[s]

    def gate_scatter():
        for s in range(2):
            a, b = mine(s)
            gate_part[s, a, b] = gate_total(s)
            ring_open(gate, s)

    def broadcast(s, step):
        return remote(
            gate_grad.at[s, fs], gate_grad.at[s, fs], gate_send.at[3], spread_recv.at[0],
            {"fs": lax.rem(fs + step, fs_size)},
        )

    def gate_collect():
        ring_close(gate)
        for s in range(2):
            a, b = mine(s)
            gate_grad[s, fs] = gate_part[s, a, b, fs]
            for step in range(1, fs_size):
                broadcast(s, step).start()

    def pre_pair(level):
        here = gate_pre.at[bits[0], bits[1]] if level == 0 else gate_pre.at[bits[0]]
        return remote(here, here, pre_send.at[level], pre_recv.at[level], {"rep": partners[1 - level]})

    def gate_product():
        arrived(gate_along, spread_recv.at[0])
        loaded("gate right", "gate left", "gate moment")
        each = gate_part.shape[4]
        for place in range(each):
            block = (2 * bits[0] + bits[1]) * each + place
            gradient = gate_grad[:, :, place].reshape(width, width)
            right_done = split_dot(gradient, gate_right[block])
            moment = BETA * gate_moment[block] + split_dot_left(gate_left[block], right_done)
            gate_pre[bits[0], bits[1], place] = moment
            sums[2] += folded_squares(gradient) * (1.0 / fs_size)
            sums[3] += folded_squares(moment)
        pre_pair(0).start()

    def gate_forward():
        pre_pair(0).wait_recv()
        pre_pair(1).start()

    def gate_finish():
        pre_pair(1).wait_recv()
        each = gate_part.shape[4]
        for block in range(blocks):
            head, place = block // each, block % each
            gate_new[block] = gate_pre[head // 2, head % 2, place]

    def cube(s, step):
        mask = masks[step] if s == 0 else masks[-1 - step]
        return remote(
            gate_held.at[s, step], gate_along.at[s, step], cube_send.at[s, step], cube_recv.at[s, step],
            {"fs": fs ^ mask},
        )

    def whole_pair(s, level):
        a, b = mine(s)
        here = gate_grad.at[s, a, b] if level == 0 else gate_grad.at[s, a]
        return remote(
            here, here, pre_send.at[2 * s + level], pre_recv.at[2 * s + level],
            {"rep": partners[1 - s if level == 0 else s]},
        )

    def cube_open():
        for s in range(2):
            gate_held[s, 0] = gate_total(s)
            cube(s, 0).start()

    def cube_add(step):
        for s in range(2):
            cube(s, step).wait_recv()
            total = gate_held[s, step] + gate_along[s, step]
            if step + 1 < len(masks):
                gate_held[s, step + 1] = total
                cube(s, step + 1).start()
            else:
                a, b = mine(s)
                gate_grad[s, a, b] = total
                whole_pair(s, 0).start()

    def whole_forward():
        for s in range(2):
            whole_pair(s, 0).wait_recv()
            whole_pair(s, 1).start()

    def whole_finish():
        for s in range(2):
            whole_pair(s, 1).wait_recv()
        loaded("gate right", "gate left", "gate moment")

        @pl.loop(0, blocks)
        def _(block):
            gradient = gate_grad[:, :, :, block].reshape(width, width)
            right_done = split_dot(gradient, gate_right[block])
            moment = BETA * gate_moment[block] + split_dot_left(gate_left[block], right_done)
            gate_new[block] = moment
            sums[2] += folded_squares(gradient) * (0.25 / fs_size)
            sums[3] += folded_squares(moment) * 0.25

    def rec_stages(k):
        return [functools.partial(f, k) for f in (open_rec, spread, fold, collect, settle, forward, finish)]

    gate_stages = [open_gate, gate_add_first]
    if by_head:
        gate_stages += [gate_scatter, functools.partial(fold, gate), gate_collect, gate_product, gate_forward, gate_finish]
    else:
        gate_stages += [cube_open, *(functools.partial(cube_add, step) for step in range(len(masks)))]
        gate_stages += [whole_forward, whole_finish]
    queue = [rec_stages(k) for k in range(len(units))]
    queue.insert(min(GATE_PLACE, len(queue)), gate_stages)

    agenda = []
    for place, stages in enumerate(queue):
        offsets = GATE_AT if stages is gate_stages else REC_AT
        for stage, action in enumerate(stages):
            offset = offsets[stage] if stage < len(offsets) else offsets[-1] + stage + 1 - len(offsets)
            agenda.append((max(0, place + offset), stage > 0, -place if stage else place, stage, action))

    def exchange_open(index):
        axes, base = groups[index], sum(counts[:index])
        me = base
        scale = 1
        for axis in reversed(axes):
            me = me + places[axis] * scale
            scale *= sizes[axis]
        slots[me] = message[...]
        for peer in members(axes):
            remote(message, slots.at[me], sum_send.at[index], sum_recv.at[index], peer).start()

    def exchange_close(index):
        base = sum(counts[:index])
        others = slots.at[base : base + counts[index] - 1]
        arrived(others, sum_recv.at[index])
        sent(others, sum_send.at[index])
        message[...] = jnp.sum(slots[base : base + counts[index]], axis=0)

    adding = {settle, gate_product, whole_finish}
    left = sum(getattr(entry[-1], "func", entry[-1]) in adding for entry in agenda)
    for tick, _, place, stage, action in sorted(agenda, key=lambda entry: entry[:4]):
        action()
        if getattr(action, "func", action) in adding:
            left -= 1
            if not left:
                for i in range(4):
                    message[i : i + 1] = jnp.sum(sums[i], axis=0, keepdims=True)
                message[4:8] = jnp.zeros((4, LANES), jnp.float32)
                exchange_open(0)

    exchange_close(0)
    for index in range(1, len(groups)):
        exchange_open(index)
        exchange_close(index)
    total = message[...]
    squares = [jnp.sum(total[i : i + 1], keepdims=True) for i in range(4)]
    rec_scale = jnp.sqrt(squares[0]) / jnp.sqrt(squares[1] + EPSILON)
    gate_scale = jnp.sqrt(squares[2]) / jnp.sqrt(squares[3] + EPSILON)
    scales[0] = jnp.broadcast_to(rec_scale, (8, LANES))
    scales[1] = jnp.broadcast_to(gate_scale, (8, LANES))

    sent(first, rec_send.at[0])
    sent(along, rec_send.at[1])
    sent(grad, rec_send.at[2])
    sent(gate_first, gate_send.at[0])
    sent(gate_second, gate_send.at[1])
    if by_head:
        sent(gate_along, gate_send.at[2])
        sent(gate_along, gate_send.at[3])
        for level in range(2):
            pre_pair(level).wait_send()
    else:
        for s in range(2):
            for step in range(len(masks)):
                cube(s, step).wait_send()
            for level in range(2):
                whole_pair(s, level).wait_send()


def update_kernel(
    rec_weight, gate_weight, rec_new, gate_new, scales,
    rec_weight_out, rec_new_out, rec_step_out, rec_copy_out,
    gate_weight_out, gate_new_out, gate_step_out, gate_copy_out,
    rec_after, rec_step, rec_copy, gate_after, gate_step, gate_copy,
    out_sem,
):
    groups = (
        (rec_weight, rec_new, rec_after, rec_step, rec_copy, rec_weight_out, rec_new_out, rec_step_out, rec_copy_out),
        (gate_weight, gate_new, gate_after, gate_step, gate_copy,
         gate_weight_out, gate_new_out, gate_step_out, gate_copy_out),
    )
    copies = []
    for group, (weight, new, after, step, copy, *outs) in enumerate(groups):
        parts = PARTS if weight.shape[0] % PARTS == 0 else 1
        size = weight.shape[0] // parts
        factor = LEARN_RATE * scales[group, 0:1, 0:1]
        for i in range(parts):
            here = slice(i * size, (i + 1) * size)
            moved = pltpu.make_async_copy(new.at[here], outs[1].at[here], out_sem.at[group, i, 1])
            moved.start()
            copies.append(moved)
        for i in range(parts):
            here = slice(i * size, (i + 1) * size)
            moment = new[here]
            taken = (factor if moment.ndim == 2 else factor[None]) * moment
            step[here] = taken
            result = weight[here] - taken
            after[here] = result
            copy[here] = result.astype(jnp.bfloat16)
            for index, source in ((0, after), (2, step), (3, copy)):
                moved = pltpu.make_async_copy(source.at[here], outs[index].at[here], out_sem.at[group, i, index])
                moved.start()
                copies.append(moved)
    for moved in copies:
        moved.wait()


def shards(fs_size, rep_size, tp_size, normed, rec_cot, conv_out, gate_cot, rec_weight, rec_moment,
           rec_right, gate_weight, gate_moment, gate_left, gate_right):
    assert rep_size == 4 and fs_size & (fs_size - 1) == 0 and fs_size >= 4
    f32 = jnp.float32
    fs_rows, columns = rec_weight.shape
    width = rec_right.shape[1]
    blocks, gate_rows = gate_weight.shape[:2]
    units = plan(fs_rows, columns // width)
    rows = fs_rows * (columns // width) // 8
    others = fs_size - 1
    cubes = fs_size.bit_length() - 1
    direct = fs_size * rep_size * tp_size <= 32
    groups, tiles = (1, fs_size * rep_size * tp_size) if direct else (3, fs_size + rep_size + tp_size)
    loads = columns // width + sum(unit[0] == 0 for unit in units) + 7
    operands = (normed, rec_cot, conv_out, gate_cot, rec_moment, rec_right, gate_moment, gate_left, gate_right)
    vmem = pl.BlockSpec(memory_space=pltpu.VMEM)
    dma = pltpu.SemaphoreType.DMA
    by_head = blocks % 4 == 0
    if by_head:
        thin = (blocks // 4, width // 2 // fs_size, width)
        piece = (fs_size, *thin)
        gate_held = None
        gate_along = pltpu.VMEM((2, others, *thin), f32)
        gate_helped = pltpu.VMEM((2, *thin), f32)
        gate_grad = pltpu.VMEM((2, *piece), f32)
        gate_pre = pltpu.VMEM((2, 2, blocks // 4, gate_rows, width), f32)
    else:
        piece = (blocks, width // 8, width)
        gate_held = pltpu.VMEM((2, cubes, *piece), f32)
        gate_along = pltpu.VMEM((2, cubes, *piece), f32)
        gate_helped = None
        gate_grad = pltpu.VMEM((2, 2, 2, *piece), f32)
        gate_pre = None
    rec_new, gate_new, scales = pl.pallas_call(
        functools.partial(kernel, fs_size, tp_size, units),
        out_shape=(
            pltpu.VMEM(rec_weight.shape, f32),
            pltpu.VMEM(gate_weight.shape, f32),
            pltpu.VMEM((2, 8, LANES), f32),
        ),
        in_specs=[pl.BlockSpec(memory_space=pltpu.HBM)] * len(operands),
        out_specs=(vmem,) * 3,
        scratch_shapes=[
            *(pltpu.VMEM(x.shape, x.dtype) for x in operands),
            pltpu.VMEM((2, 2, 2, fs_size, rows, width), f32),
            pltpu.VMEM((2, 2, fs_size, rows, width), f32),
            pltpu.VMEM((2, rows, width), f32),
            pltpu.VMEM((2, others, 2, rows, width), f32),
            pltpu.VMEM((2, 2, rows, width), f32),
            pltpu.VMEM((2, 2, 2, rows, width), f32),
            pltpu.VMEM((2, 2, 2, *piece), f32),
            pltpu.VMEM((2, 2, *piece), f32),
            pltpu.VMEM((2, *piece), f32),
            gate_held,
            gate_along,
            gate_helped,
            gate_grad,
            gate_pre,
            pltpu.VMEM((4, 8, LANES), f32),
            pltpu.VMEM((8, LANES), f32),
            pltpu.VMEM((tiles, 8, LANES), f32),
            dma((loads,)),
            dma((3,)),
            dma((len(units), 4)),
            dma((len(units) + 1,)),
            dma((len(units) + 1,)),
            dma((4,)),
            dma((2,)),
            dma((1,)),
            dma((4,)),
            dma((4,)),
            None if by_head else dma((2, cubes)),
            None if by_head else dma((2, cubes)),
            dma((groups,)),
            dma((groups,)),
        ],
        compiler_params=pltpu.CompilerParams(
            collective_id=0, has_side_effects=True, vmem_limit_bytes=44 * 1024 * 1024
        ),
    )(*(pltpu.with_memory_space_constraint(x, pltpu.HBM) for x in operands))

    return update(rec_weight, gate_weight, rec_new, gate_new, scales)


def update(rec_weight, gate_weight, rec_new, gate_new, scales):
    vmem = pl.BlockSpec(memory_space=pltpu.VMEM)
    hbm = pl.BlockSpec(memory_space=pltpu.HBM)
    f32, bf16 = jnp.float32, jnp.bfloat16
    weights = (rec_weight, gate_weight)
    shapes = [jax.ShapeDtypeStruct(w.shape, t) for w in weights for t in (f32, f32, f32, bf16)]
    return pl.pallas_call(
        update_kernel,
        out_shape=shapes,
        in_specs=[vmem] * 5,
        out_specs=[hbm] * 8,
        scratch_shapes=[
            *(pltpu.VMEM(w.shape, t) for w in weights for t in (f32, f32, bf16)),
            pltpu.SemaphoreType.DMA((2, PARTS, 4)),
        ],
        compiler_params=pltpu.CompilerParams(vmem_limit_bytes=16 * 1024 * 1024),
    )(
        *(pltpu.with_memory_space_constraint(x, pltpu.VMEM) for x in (rec_weight, gate_weight, rec_new, gate_new, scales))
    )


def solution(mesh):
    in_specs = (
        P(("fs", "rep"), None),
        P(("fs", "rep"), "tp"),
        P(("fs", "rep"), "tp"),
        P(("fs", "rep"), "tp"),
        P("fs", "tp"),
        P("fs", "tp"),
        P("tp", None),
        P("tp", "fs", None),
        P("tp", "fs", None),
        P("tp", "fs", None),
        P("tp", None, None),
    )
    out_specs = (P("fs", "tp"),) * 4 + (P("tp", "fs", None),) * 4
    body = functools.partial(shards, mesh.shape["fs"], mesh.shape["rep"], mesh.shape["tp"])
    return jax.shard_map(body, mesh=mesh, in_specs=in_specs, out_specs=out_specs, check_vma=False)
```

```python
import functools
import itertools
import math

import jax
import jax.numpy as jnp
from jax import lax
from jax.experimental import pallas as pl
from jax.experimental.pallas import tpu as pltpu
from jax.sharding import PartitionSpec as P

BETA = 0.9
LEARN_RATE = 0.02
EPSILON = 1e-06
MESH = pl.DeviceIdType.MESH
LANES = 128
PARTS = 4
LATE, MIDDLE, FINAL = range(3)
ALONG_FIRST = 0
ALONG_LAST = 3
GATE_PLACE = 5
OPEN_AT = (0, 0, 1, 2, 4)
REC_AT = (0, 1, 2, 3, 4, 5, 6)
GATE_AT = (0, 1, 2, 3, 4, 6, 8, 10)


def split_dot(value, factor):
    high = value.astype(jnp.bfloat16)
    low = (value - high.astype(jnp.float32)).astype(jnp.bfloat16)
    return jnp.dot(high, factor, preferred_element_type=jnp.float32) + jnp.dot(
        low, factor, preferred_element_type=jnp.float32
    )


def split_dot_left(factor, value):
    high = value.astype(jnp.bfloat16)
    low = (value - high.astype(jnp.float32)).astype(jnp.bfloat16)
    return jnp.dot(factor, high, preferred_element_type=jnp.float32) + jnp.dot(
        factor, low, preferred_element_type=jnp.float32
    )


def token_dot(left, right):
    return lax.dot_general(left, right, (((0,), (0,)), ((), ())), preferred_element_type=jnp.float32)


def folded_squares(value):
    squares = value * value
    rows, width = squares.shape
    total = jnp.sum(squares.reshape(rows // 8, 8, width), axis=0)
    result = total[:, :LANES]
    for start in range(LANES, width, LANES):
        result = result + total[:, start : start + LANES]
    return result


def plan(fs_rows, column_count):
    units = []
    for column in range(column_count):
        sizes = [256] * (fs_rows // 256) or [fs_rows]
        if len(sizes) > 1 and column == 0:
            sizes = [128, 128] + sizes[1:]
        if len(sizes) > 1 and column == column_count - 1:
            sizes = sizes[:-1] + [128, 128]
        start = 0
        for size in sizes:
            units.append((column, start, size, (column * fs_rows + start) // 8))
            start += size
    if len(units) > 4:
        kinds = [LATE] * ALONG_FIRST + [MIDDLE] * (len(units) - ALONG_FIRST - ALONG_LAST) + [FINAL] * ALONG_LAST
    else:
        kinds = [MIDDLE] * len(units)
    return units, kinds


def span_of(units, kinds, wanted):
    chosen = [unit for unit, kind in zip(units, kinds) if kind in wanted]
    return slice(chosen[0][3], chosen[-1][3] + chosen[-1][2] // 8) if chosen else None


def kernel(
    fs_size, tp_size, units, kinds,
    normed_hbm, rec_cot_hbm, conv_hbm, gate_cot_hbm, rec_moment_hbm, rec_right_hbm, gate_moment_hbm, gate_left_hbm,
    gate_right_hbm,
    rec_new, gate_new, scales,
    normed, rec_cot, conv_out, gate_cot, rec_moment, rec_right, gate_moment, gate_left, gate_right,
    part, first, second, along, helped, grad, wide_along, wide_helped, thick_second,
    gate_part, gate_first, gate_second, gate_held, gate_along, gate_helped, gate_grad, gate_pre,
    sums, message, slots,
    in_sem, rec_send, kind_send, pair_recv, ring_recv, help_recv,
    gate_send, gate_recv, spread_recv, pre_send, pre_recv, cube_send, cube_recv, sum_send, sum_recv,
):
    fs, rep, tp = lax.axis_index("fs"), lax.axis_index("rep"), lax.axis_index("tp")
    bits = (lax.rem(rep, 2), rep // 2)
    partners = (rep + 1 - 2 * bits[0], rep + 2 - 4 * bits[1])
    width = part.shape[-1]
    fs_rows = rec_moment.shape[0]
    blocks = gate_moment.shape[0]
    masks = [2**i - 1 for i in range(1, fs_size.bit_length())]
    by_head = gate_pre is not None
    last = fs_size - 1
    gate = len(units)

    copies = []
    waits = {}

    def load(name, source, target, sem=None):
        sem = in_sem.at[len(waits)] if sem is None else sem
        copies.append(pltpu.make_async_copy(source, target, sem))
        waits.setdefault(name, (target, sem))
        return sem

    def column_of(k):
        return slice(units[k][0] * width, (units[k][0] + 1) * width)

    def fetch_columns(column):
        span = slice(column * width, (column + 1) * width)
        load(("cot", column), rec_cot_hbm.at[:, span], rec_cot.at[:, span])

    fetch_columns(0)
    for column, start, size, _ in units:
        if column == 0:
            sem = None
            for owner in range(fs_size):
                span = slice(owner * fs_rows + start, owner * fs_rows + start + size)
                sem = load(("normed", start), normed_hbm.at[:, span], normed.at[:, span], sem)
            waits["normed", start] = (normed.at[:, 0 : fs_size * size], sem)
            if start == 0:
                load("conv", conv_hbm, conv_out)
                load("gate", gate_cot_hbm, gate_cot)
    for column in range(1, units[-1][0] + 1):
        fetch_columns(column)
    load("right", rec_right_hbm, rec_right)
    load("moment", rec_moment_hbm, rec_moment)
    load("gate right", gate_right_hbm, gate_right)
    load("gate left", gate_left_hbm, gate_left)
    load("gate moment", gate_moment_hbm, gate_moment)
    for copy in copies:
        copy.start()

    def loaded(*names):
        for name in names:
            if name in waits:
                whole, sem = waits.pop(name)
                pltpu.make_async_copy(whole, whole, sem).wait()

    sizes = {"fs": fs_size, "rep": 4, "tp": tp_size}
    places = {"fs": fs, "rep": rep, "tp": tp}
    direct = fs_size * tp_size <= 8
    groups = [("fs", "tp"), ("rep",)] if direct else [("fs",), ("tp",), ("rep",)]
    counts = [math.prod(sizes[axis] for axis in axes) for axes in groups]

    def members(axes):
        return [
            {axis: lax.rem(places[axis] + move, sizes[axis]) for axis, move in zip(axes, moves)}
            for moves in itertools.product(*(range(sizes[axis]) for axis in axes))
            if any(moves)
        ]

    barrier = pltpu.get_barrier_semaphore()
    greeted = [peer for axes in groups for peer in members(axes)]
    for peer in greeted:
        pl.semaphore_signal(barrier, inc=1, device_id=peer, device_id_type=MESH)
    sums[...] = jnp.zeros_like(sums)

    def remote(source, target, send, recv, peer):
        return pltpu.make_async_remote_copy(
            src_ref=source, dst_ref=target, send_sem=send, recv_sem=recv,
            device_id=peer, device_id_type=MESH,
        )

    def arrived(whole, recv):
        remote(whole, whole, rec_send.at[0], recv, {"rep": partners[0]}).wait_recv()

    def sent(whole, send):
        remote(whole, whole, send, pair_recv.at[0, 0], {"rep": partners[0]}).wait_send()

    def mine(s):
        return bits[s], bits[1 - s]

    def rows_of(k):
        return slice(units[k][3], units[k][3] + units[k][2] // 8)

    def first_pair(k, s):
        a, _ = mine(s)
        here = rows_of(k)
        if kinds[k] == LATE:
            source, target, sem = part.at[s, 1 - a, :, fs, here], first.at[s, :, 0, here], kind_send.at[0]
        else:
            source, target, sem = part.at[s, 1 - a, :, :, here], first.at[s, :, :, here], rec_send.at[0]
        return remote(source, target, sem, pair_recv.at[k, 0], {"rep": partners[s]})

    def second_pair(k, s):
        a, b = mine(s)
        here = rows_of(k)
        if kinds[k] == FINAL:
            source, target, sem = part.at[s, a, 1 - b, :, here], thick_second.at[s, :, thick(k)], kind_send.at[1]
        else:
            source, target, sem = part.at[s, a, 1 - b, fs, here], second.at[s, here], rec_send.at[2]
        return remote(source, target, sem, pair_recv.at[k, 1], {"rep": partners[1 - s]})

    def gather_pair(k, s, level):
        a, b = mine(s)
        if level == 0:
            here = grad.at[s, a, b, rows_of(k)]
        else:
            here = grad.at[s, a, :, rows_of(k)]
        sem = kind_send.at[2 + level] if kinds[k] == FINAL else rec_send.at[2]
        return remote(here, here, sem, pair_recv.at[k, 2 + level], {"rep": partners[1 - s if level == 0 else s]})

    def thick(k):
        begin = units[k][3] - span_of(units, kinds, (FINAL,)).start
        return slice(begin, begin + units[k][2] // 8)

    def chunk(k, s, owner):
        a, b = mine(s)
        if k == gate:
            return gate_part.at[s, a, b, owner]
        if kinds[k] == LATE:
            return part.at[s, :, :, owner, rows_of(k)]
        return part.at[s, a, b if kinds[k] == FINAL else slice(None), owner, rows_of(k)]

    def ring_slots(k, s, steps):
        if k == gate:
            return gate_along.at[s, steps]
        if kinds[k] == LATE:
            return wide_along.at[s, steps, :, :, rows_of(k)]
        return along.at[s, steps, 0 if kinds[k] == FINAL else slice(None), rows_of(k)]

    def ring_slot(k, s, step):
        return ring_slots(k, s, step - 1)

    def help_slot(k, s):
        if k == gate:
            return gate_helped.at[s]
        if kinds[k] == LATE:
            return wide_helped.at[s, :, :, rows_of(k)]
        return helped.at[s, 0 if kinds[k] == FINAL else slice(None), rows_of(k)]

    def ring_sem(k):
        if k == gate:
            return gate_send.at[2]
        return rec_send.at[1] if kinds[k] == MIDDLE else kind_send.at[4 if kinds[k] == LATE else 5]

    def ring(k, s, step):
        peer = lax.rem(fs + step, fs_size)
        return remote(chunk(k, s, peer), ring_slot(k, s, step), ring_sem(k), ring_recv.at[k], {"fs": peer})

    def helper(k, s):
        return remote(
            chunk(k, s, last - fs), help_slot(k, s), ring_sem(k), help_recv.at[k],
            {"fs": jnp.where(fs == 0, 1, last - 1)},
        )

    at_end = (fs == 0) | (fs == last)
    beside = (fs == 1) | (fs == last - 1)
    fold_step = jnp.where(fs == 1, last - 1, 2)

    def when(condition, action):
        if condition is None:
            action()
        else:
            pl.when(condition)(action)

    def sends(step):
        skip = []
        if step == last:
            skip.append(fs == 0)
        if step == 1:
            skip.append(fs == last)
        if step == last - 1:
            skip.append(fs == 1)
        if step == 2:
            skip.append(fs == last - 1)
        return jnp.logical_not(functools.reduce(jnp.logical_or, skip)) if skip else None

    def receives(step):
        if step == last:
            return fs != last
        if step == 1:
            return fs != 0
        return None

    def ring_open(k, s):
        pl.when(at_end)(lambda: helper(k, s).start())
        for step in range(1, fs_size):
            when(sends(step), lambda step=step: ring(k, s, step).start())

    def fold(k):
        @pl.when(beside)
        def _():
            arrived(help_slot(k, slice(None)), help_recv.at[k])
            for s in range(2):
                whole = chunk(k, s, lax.rem(fs + fold_step, fs_size))
                whole[...] += help_slot(k, s)[...]
                ring(k, s, fold_step).start()

    def ring_close(k):
        def slots_of(count):
            return ring_slots(k, slice(None), slice(0, count))

        pl.when(at_end)(lambda: arrived(slots_of(last - 1), ring_recv.at[k]))
        pl.when(jnp.logical_not(at_end))(lambda: arrived(slots_of(last), ring_recv.at[k]))
        for s in range(2):
            own = chunk(k, s, fs)
            for step in range(1, fs_size):
                def take(own=own, s=s, step=step):
                    own[...] += ring_slot(k, s, step)[...]

                when(receives(step), take)

    def product(k):
        column, start, size, _ = units[k]
        loaded(("cot", column))
        loaded(("normed", start))

        @pl.loop(0, fs_size)
        def _(owner):
            begin = pl.multiple_of(owner * fs_rows + start, 128)
            term = token_dot(normed[:, pl.ds(begin, size)], rec_cot[:, column_of(k)])
            part[:, :, :, owner, rows_of(k)] = term.reshape(2, 2, 2, size // 8, width)

    def open_rec(k):
        product(k)
        if k == 0:
            pl.semaphore_wait(barrier, len(greeted))
        for s in range(2):
            if kinds[k] == LATE:
                ring_open(k, s)
            else:
                first_pair(k, s).start()

    def add_first(k, s):
        a, _ = mine(s)

        @pl.loop(0, fs_size)
        def _(owner):
            for b in range(2):
                part[s, a, b, owner, rows_of(k)] += first[s, b, owner, rows_of(k)]

    def spread(k):
        arrived(first.at[:, :, :, rows_of(k)], pair_recv.at[k, 0])
        for s in range(2):
            add_first(k, s)
            ring_open(k, s)

    def collect(k):
        ring_close(k)
        for s in range(2):
            second_pair(k, s).start()

    def collect_late(k):
        ring_close(k)
        for s in range(2):
            first_pair(k, s).start()

    def add_late(k):
        arrived(first.at[:, :, 0, rows_of(k)], pair_recv.at[k, 0])
        for s in range(2):
            a, _ = mine(s)
            part[s, a, :, fs, rows_of(k)] += first[s, :, 0, rows_of(k)]
            second_pair(k, s).start()

    def halve(k):
        arrived(first.at[:, :, :, rows_of(k)], pair_recv.at[k, 0])
        for s in range(2):
            add_first(k, s)
            second_pair(k, s).start()

    def spread_final(k):
        arrived(thick_second.at[:, :, thick(k)], pair_recv.at[k, 1])
        for s in range(2):
            a, b = mine(s)
            part[s, a, b, :, rows_of(k)] += thick_second[s, :, thick(k)]
            ring_open(k, s)

    def settle(k):
        loaded("right", "moment")
        if kinds[k] == FINAL:
            ring_close(k)
        else:
            arrived(second.at[:, rows_of(k)], pair_recv.at[k, 1])
        _, start, size, _ = units[k]
        rows = size // 8
        gradients, moments = [], []
        for s in range(2):
            a, b = mine(s)
            quarter = part[s, a, b, fs, rows_of(k)]
            gradients.append(quarter if kinds[k] == FINAL else quarter + second[s, rows_of(k)])
            begin = pl.multiple_of(start + (4 * s + 2 * a + b) * rows, 8)
            moments.append(rec_moment[pl.ds(begin, rows), column_of(k)])
        gradient = jnp.concatenate(gradients, axis=0)
        moment = BETA * jnp.concatenate(moments, axis=0) + split_dot(gradient, rec_right[column_of(k), :])
        for s in range(2):
            a, b = mine(s)
            grad[s, a, b, rows_of(k)] = moment[s * rows : (s + 1) * rows]
            gather_pair(k, s, 0).start()
        sums[0] += folded_squares(gradient)
        sums[1] += folded_squares(moment)

    def forward(k):
        arrived(grad.at[0, :, 0, rows_of(k)], pair_recv.at[k, 2])
        for s in range(2):
            gather_pair(k, s, 1).start()

    def finish(k):
        arrived(grad.at[0, :, :, rows_of(k)], pair_recv.at[k, 3])
        _, start, size, _ = units[k]
        rec_new[start : start + size, column_of(k)] = grad[:, :, :, rows_of(k)].reshape(size, width)

    def gate_pair(s, index):
        a, b = mine(s)
        source, target = (gate_part.at[s, 1 - a], gate_first) if index == 0 else (gate_part.at[s, a, 1 - b], gate_second)
        return remote(
            source, target.at[s], gate_send.at[index], gate_recv.at[index],
            {"rep": partners[s if index == 0 else 1 - s]},
        )

    def open_gate():
        loaded("conv", "gate")

        @pl.loop(0, blocks)
        def _(block):
            columns = pl.ds(pl.multiple_of(block * width, width), width)
            term = token_dot(conv_out[:, columns], gate_cot[:, columns])
            if by_head:
                each, thin = gate_part.shape[4], gate_part.shape[5]
                head, place = block // each, lax.rem(block, each)
                halves = term.reshape(2, fs_size, thin, width)
                gate_part[0, head // 2, lax.rem(head, 2), :, place] = halves[0]
                gate_part[1, lax.rem(head, 2), head // 2, :, place] = halves[1]
            else:
                gate_part[:, :, :, block] = term.reshape(2, 2, 2, gate_part.shape[4], width)

        for s in range(2):
            gate_pair(s, 0).start()

    def gate_add_first():
        arrived(gate_first, gate_recv.at[0])
        for s in range(2):
            a, _ = mine(s)
            gate_part[s, a] += gate_first[s]
            gate_pair(s, 1).start()

    def gate_total(s):
        if s == 0:
            arrived(gate_second, gate_recv.at[1])
        a, b = mine(s)
        return gate_part[s, a, b] + gate_second[s]

    def gate_scatter():
        for s in range(2):
            a, b = mine(s)
            gate_part[s, a, b] = gate_total(s)
            ring_open(gate, s)

    def broadcast(s, step):
        return remote(
            gate_grad.at[s, fs], gate_grad.at[s, fs], gate_send.at[3], spread_recv.at[0],
            {"fs": lax.rem(fs + step, fs_size)},
        )

    def gate_collect():
        ring_close(gate)
        for s in range(2):
            a, b = mine(s)
            gate_grad[s, fs] = gate_part[s, a, b, fs]
            for step in range(1, fs_size):
                broadcast(s, step).start()

    def pre_pair(level):
        here = gate_pre.at[bits[0], bits[1]] if level == 0 else gate_pre.at[bits[0]]
        return remote(here, here, pre_send.at[level], pre_recv.at[level], {"rep": partners[1 - level]})

    def gate_product():
        arrived(gate_along, spread_recv.at[0])
        loaded("gate right", "gate left", "gate moment")
        each = gate_part.shape[4]
        for place in range(each):
            block = (2 * bits[0] + bits[1]) * each + place
            gradient = gate_grad[:, :, place].reshape(width, width)
            right_done = split_dot(gradient, gate_right[block])
            moment = BETA * gate_moment[block] + split_dot_left(gate_left[block], right_done)
            gate_pre[bits[0], bits[1], place] = moment
            sums[2] += folded_squares(gradient) * (1.0 / fs_size)
            sums[3] += folded_squares(moment)
        pre_pair(0).start()

    def gate_forward():
        pre_pair(0).wait_recv()
        pre_pair(1).start()

    def gate_finish():
        pre_pair(1).wait_recv()
        each = gate_part.shape[4]
        for block in range(blocks):
            head, place = block // each, block % each
            gate_new[block] = gate_pre[head // 2, head % 2, place]

    def cube(s, step):
        mask = masks[step] if s == 0 else masks[-1 - step]
        return remote(
            gate_held.at[s, step], gate_along.at[s, step], cube_send.at[s, step], cube_recv.at[s, step],
            {"fs": fs ^ mask},
        )

    def whole_pair(s, level):
        a, b = mine(s)
        here = gate_grad.at[s, a, b] if level == 0 else gate_grad.at[s, a]
        return remote(
            here, here, pre_send.at[2 * s + level], pre_recv.at[2 * s + level],
            {"rep": partners[1 - s if level == 0 else s]},
        )

    def cube_open():
        for s in range(2):
            gate_held[s, 0] = gate_total(s)
            cube(s, 0).start()

    def cube_add(step):
        for s in range(2):
            cube(s, step).wait_recv()
            total = gate_held[s, step] + gate_along[s, step]
            if step + 1 < len(masks):
                gate_held[s, step + 1] = total
                cube(s, step + 1).start()
            else:
                a, b = mine(s)
                gate_grad[s, a, b] = total
                whole_pair(s, 0).start()

    def whole_forward():
        for s in range(2):
            whole_pair(s, 0).wait_recv()
            whole_pair(s, 1).start()

    def whole_finish():
        for s in range(2):
            whole_pair(s, 1).wait_recv()
        loaded("gate right", "gate left", "gate moment")

        @pl.loop(0, blocks)
        def _(block):
            gradient = gate_grad[:, :, :, block].reshape(width, width)
            right_done = split_dot(gradient, gate_right[block])
            moment = BETA * gate_moment[block] + split_dot_left(gate_left[block], right_done)
            gate_new[block] = moment
            sums[2] += folded_squares(gradient) * (0.25 / fs_size)
            sums[3] += folded_squares(moment) * 0.25

    def rec_stages(k):
        middle = {
            LATE: (fold, collect_late, add_late), MIDDLE: (spread, fold, collect), FINAL: (halve, spread_final, fold)
        }[kinds[k]]
        return [functools.partial(f, k) for f in (open_rec, *middle, settle, forward, finish)]

    gate_stages = [open_gate, gate_add_first]
    if by_head:
        gate_stages += [gate_scatter, functools.partial(fold, gate), gate_collect, gate_product, gate_forward, gate_finish]
    else:
        gate_stages += [cube_open, *(functools.partial(cube_add, step) for step in range(len(masks)))]
        gate_stages += [whole_forward, whole_finish]
    queue = [rec_stages(k) for k in range(len(units))]
    queue.insert(min(GATE_PLACE, len(queue)), gate_stages)

    agenda = []
    for place, stages in enumerate(queue):
        offsets = GATE_AT if stages is gate_stages else REC_AT
        for stage, action in enumerate(stages):
            offset = offsets[stage] if stage < len(offsets) else offsets[-1] + stage + 1 - len(offsets)
            tick = OPEN_AT[place] if stage == 0 and place < len(OPEN_AT) else max(0, place + offset)
            agenda.append((tick, stage > 0, -place if stage else place, stage, action))

    def exchange_open(index):
        axes, base = groups[index], sum(counts[:index])
        me = base
        scale = 1
        for axis in reversed(axes):
            me = me + places[axis] * scale
            scale *= sizes[axis]
        slots[me] = message[...]
        for peer in members(axes):
            remote(message, slots.at[me], sum_send.at[index], sum_recv.at[index], peer).start()

    def exchange_close(index):
        base = sum(counts[:index])
        others = slots.at[base : base + counts[index] - 1]
        arrived(others, sum_recv.at[index])
        sent(others, sum_send.at[index])
        message[...] = jnp.sum(slots[base : base + counts[index]], axis=0)

    adding = {settle, gate_product, whole_finish}
    left = sum(getattr(entry[-1], "func", entry[-1]) in adding for entry in agenda)
    for tick, _, place, stage, action in sorted(agenda, key=lambda entry: entry[:4]):
        action()
        if getattr(action, "func", action) in adding:
            left -= 1
            if not left:
                for i in range(4):
                    message[i : i + 1] = jnp.sum(sums[i], axis=0, keepdims=True)
                message[4:8] = jnp.zeros((4, LANES), jnp.float32)
                exchange_open(0)
        elif left == 0:
            exchange_close(0)
            exchange_open(1)
            left = None

    if left is not None:
        exchange_close(0)
        exchange_open(1)
    for index in range(1, len(groups)):
        exchange_close(index)
        if index + 1 < len(groups):
            exchange_open(index + 1)
    total = message[...]
    squares = [jnp.sum(total[i : i + 1], keepdims=True) for i in range(4)]
    rec_scale = jnp.sqrt(squares[0]) / jnp.sqrt(squares[1] + EPSILON)
    gate_scale = jnp.sqrt(squares[2]) / jnp.sqrt(squares[3] + EPSILON)
    scales[0] = jnp.broadcast_to(rec_scale, (8, LANES))
    scales[1] = jnp.broadcast_to(gate_scale, (8, LANES))

    early = span_of(units, kinds, (MIDDLE, FINAL))
    sent(first.at[:, :, :, early], rec_send.at[0])
    sent(along.at[:, :, :, span_of(units, kinds, (MIDDLE,))], rec_send.at[1])
    sent(grad.at[:, :, :, span_of(units, kinds, (LATE, MIDDLE))], rec_send.at[2])
    if LATE in kinds:
        sent(first.at[:, :, 0, span_of(units, kinds, (LATE,))], kind_send.at[0])
        sent(wide_along, kind_send.at[4])
    if FINAL in kinds:
        sent(thick_second, kind_send.at[1])
        final = span_of(units, kinds, (FINAL,))
        sent(grad.at[0, :, 0, final], kind_send.at[2])
        sent(grad.at[0, :, :, final], kind_send.at[3])
        sent(along.at[:, :, 0, final], kind_send.at[5])
    sent(gate_first, gate_send.at[0])
    sent(gate_second, gate_send.at[1])
    if by_head:
        sent(gate_along, gate_send.at[2])
        sent(gate_along, gate_send.at[3])
        for level in range(2):
            pre_pair(level).wait_send()
    else:
        for s in range(2):
            for step in range(len(masks)):
                cube(s, step).wait_send()
            for level in range(2):
                whole_pair(s, level).wait_send()


def update_kernel(
    rec_weight, gate_weight, rec_new, gate_new, scales,
    rec_weight_out, rec_new_out, rec_step_out, rec_copy_out,
    gate_weight_out, gate_new_out, gate_step_out, gate_copy_out,
    rec_after, rec_step, rec_copy, gate_after, gate_step, gate_copy,
    out_sem,
):
    groups = (
        (rec_weight, rec_new, rec_after, rec_step, rec_copy, rec_weight_out, rec_new_out, rec_step_out, rec_copy_out),
        (gate_weight, gate_new, gate_after, gate_step, gate_copy,
         gate_weight_out, gate_new_out, gate_step_out, gate_copy_out),
    )
    copies = []
    for group, (weight, new, after, step, copy, *outs) in enumerate(groups):
        parts = PARTS if weight.shape[0] % PARTS == 0 else 1
        size = weight.shape[0] // parts
        factor = LEARN_RATE * scales[group, 0:1, 0:1]
        for i in range(parts):
            here = slice(i * size, (i + 1) * size)
            moved = pltpu.make_async_copy(new.at[here], outs[1].at[here], out_sem.at[group, i, 1])
            moved.start()
            copies.append(moved)
        for i in range(parts):
            here = slice(i * size, (i + 1) * size)
            moment = new[here]
            taken = (factor if moment.ndim == 2 else factor[None]) * moment
            step[here] = taken
            result = weight[here] - taken
            after[here] = result
            copy[here] = result.astype(jnp.bfloat16)
            for index, source in ((0, after), (2, step), (3, copy)):
                moved = pltpu.make_async_copy(source.at[here], outs[index].at[here], out_sem.at[group, i, index])
                moved.start()
                copies.append(moved)
    for moved in copies:
        moved.wait()


def shards(fs_size, rep_size, tp_size, normed, rec_cot, conv_out, gate_cot, rec_weight, rec_moment,
           rec_right, gate_weight, gate_moment, gate_left, gate_right):
    assert rep_size == 4 and fs_size & (fs_size - 1) == 0 and fs_size >= 4
    f32 = jnp.float32
    fs_rows, columns = rec_weight.shape
    width = rec_right.shape[1]
    blocks, gate_rows = gate_weight.shape[:2]
    units, kinds = plan(fs_rows, columns // width)
    late_span, final_span = span_of(units, kinds, (LATE,)), span_of(units, kinds, (FINAL,))
    late, final = (span.stop - span.start if span else None for span in (late_span, final_span))
    rows = fs_rows * (columns // width) // 8
    others = fs_size - 1
    cubes = fs_size.bit_length() - 1
    groups, tiles = (2, fs_size * tp_size + rep_size) if fs_size * tp_size <= 8 else (3, fs_size + tp_size + rep_size)
    loads = columns // width + sum(unit[0] == 0 for unit in units) + 7
    operands = (normed, rec_cot, conv_out, gate_cot, rec_moment, rec_right, gate_moment, gate_left, gate_right)
    vmem = pl.BlockSpec(memory_space=pltpu.VMEM)
    dma = pltpu.SemaphoreType.DMA
    by_head = blocks % 4 == 0
    if by_head:
        thin = (blocks // 4, width // 2 // fs_size, width)
        piece = (fs_size, *thin)
        gate_held = None
        gate_along = pltpu.VMEM((2, others, *thin), f32)
        gate_helped = pltpu.VMEM((2, *thin), f32)
        gate_grad = pltpu.VMEM((2, *piece), f32)
        gate_pre = pltpu.VMEM((2, 2, blocks // 4, gate_rows, width), f32)
    else:
        piece = (blocks, width // 8, width)
        gate_held = pltpu.VMEM((2, cubes, *piece), f32)
        gate_along = pltpu.VMEM((2, cubes, *piece), f32)
        gate_helped = None
        gate_grad = pltpu.VMEM((2, 2, 2, *piece), f32)
        gate_pre = None
    rec_new, gate_new, scales = pl.pallas_call(
        functools.partial(kernel, fs_size, tp_size, units, kinds),
        out_shape=(
            pltpu.VMEM(rec_weight.shape, f32),
            pltpu.VMEM(gate_weight.shape, f32),
            pltpu.VMEM((2, 8, LANES), f32),
        ),
        in_specs=[pl.BlockSpec(memory_space=pltpu.HBM)] * len(operands),
        out_specs=(vmem,) * 3,
        scratch_shapes=[
            *(pltpu.VMEM(x.shape, x.dtype) for x in operands),
            pltpu.VMEM((2, 2, 2, fs_size, rows, width), f32),
            pltpu.VMEM((2, 2, fs_size, rows, width), f32),
            pltpu.VMEM((2, rows, width), f32),
            pltpu.VMEM((2, others, 2, rows, width), f32),
            pltpu.VMEM((2, 2, rows, width), f32),
            pltpu.VMEM((2, 2, 2, rows, width), f32),
            late and pltpu.VMEM((2, others, 2, 2, late, width), f32),
            late and pltpu.VMEM((2, 2, 2, late, width), f32),
            final and pltpu.VMEM((2, fs_size, final, width), f32),
            pltpu.VMEM((2, 2, 2, *piece), f32),
            pltpu.VMEM((2, 2, *piece), f32),
            pltpu.VMEM((2, *piece), f32),
            gate_held,
            gate_along,
            gate_helped,
            gate_grad,
            gate_pre,
            pltpu.VMEM((4, 8, LANES), f32),
            pltpu.VMEM((8, LANES), f32),
            pltpu.VMEM((tiles, 8, LANES), f32),
            dma((loads,)),
            dma((3,)),
            dma((6,)),
            dma((len(units), 4)),
            dma((len(units) + 1,)),
            dma((len(units) + 1,)),
            dma((4,)),
            dma((2,)),
            dma((1,)),
            dma((4,)),
            dma((4,)),
            None if by_head else dma((2, cubes)),
            None if by_head else dma((2, cubes)),
            dma((groups,)),
            dma((groups,)),
        ],
        compiler_params=pltpu.CompilerParams(
            collective_id=0, has_side_effects=True, vmem_limit_bytes=44 * 1024 * 1024
        ),
    )(*(pltpu.with_memory_space_constraint(x, pltpu.HBM) for x in operands))

    return update(rec_weight, gate_weight, rec_new, gate_new, scales)


def update(rec_weight, gate_weight, rec_new, gate_new, scales):
    vmem = pl.BlockSpec(memory_space=pltpu.VMEM)
    hbm = pl.BlockSpec(memory_space=pltpu.HBM)
    f32, bf16 = jnp.float32, jnp.bfloat16
    weights = (rec_weight, gate_weight)
    shapes = [jax.ShapeDtypeStruct(w.shape, t) for w in weights for t in (f32, f32, f32, bf16)]
    return pl.pallas_call(
        update_kernel,
        out_shape=shapes,
        in_specs=[vmem] * 5,
        out_specs=[hbm] * 8,
        scratch_shapes=[
            *(pltpu.VMEM(w.shape, t) for w in weights for t in (f32, f32, bf16)),
            pltpu.SemaphoreType.DMA((2, PARTS, 4)),
        ],
        compiler_params=pltpu.CompilerParams(vmem_limit_bytes=16 * 1024 * 1024),
    )(
        *(pltpu.with_memory_space_constraint(x, pltpu.VMEM) for x in (rec_weight, gate_weight, rec_new, gate_new, scales))
    )


def solution(mesh):
    in_specs = (
        P(("fs", "rep"), None),
        P(("fs", "rep"), "tp"),
        P(("fs", "rep"), "tp"),
        P(("fs", "rep"), "tp"),
        P("fs", "tp"),
        P("fs", "tp"),
        P("tp", None),
        P("tp", "fs", None),
        P("tp", "fs", None),
        P("tp", "fs", None),
        P("tp", None, None),
    )
    out_specs = (P("fs", "tp"),) * 4 + (P("tp", "fs", None),) * 4
    body = functools.partial(shards, mesh.shape["fs"], mesh.shape["rep"], mesh.shape["tp"])
    return jax.shard_map(body, mesh=mesh, in_specs=in_specs, out_specs=out_specs, check_vma=False)
```

```python
import functools
import itertools
import math

import jax
import jax.numpy as jnp
from jax import lax
from jax.experimental import pallas as pl
from jax.experimental.pallas import tpu as pltpu
from jax.sharding import PartitionSpec as P

BETA = 0.9
LEARN_RATE = 0.02
EPSILON = 1e-06
MESH = pl.DeviceIdType.MESH
LANES = 128
PARTS = 4
LATE, MIDDLE, FINAL = range(3)
ALONG_FIRST = 0
ALONG_LAST = 3
GATE_PLACE = 5
OPEN_AT = (0, 0, 1, 2, 4)
REC_AT = (0, 1, 2, 3, 4, 5, 6)
GATE_AT = (0, 1, 2, 3, 4, 6, 8, 10)


def split_dot(value, factor):
    high = value.astype(jnp.bfloat16)
    low = (value - high.astype(jnp.float32)).astype(jnp.bfloat16)
    return jnp.dot(high, factor, preferred_element_type=jnp.float32) + jnp.dot(
        low, factor, preferred_element_type=jnp.float32
    )


def split_dot_left(factor, value):
    high = value.astype(jnp.bfloat16)
    low = (value - high.astype(jnp.float32)).astype(jnp.bfloat16)
    return jnp.dot(factor, high, preferred_element_type=jnp.float32) + jnp.dot(
        factor, low, preferred_element_type=jnp.float32
    )


def token_dot(left, right):
    return lax.dot_general(left, right, (((0,), (0,)), ((), ())), preferred_element_type=jnp.float32)


def folded_squares(value):
    squares = value * value
    rows, width = squares.shape
    total = jnp.sum(squares.reshape(rows // 8, 8, width), axis=0)
    result = total[:, :LANES]
    for start in range(LANES, width, LANES):
        result = result + total[:, start : start + LANES]
    return result


def plan(fs_rows, column_count):
    units = []
    for column in range(column_count):
        sizes = [256] * (fs_rows // 256) or [fs_rows]
        if len(sizes) > 1 and column == 0:
            sizes = [128, 128] + sizes[1:]
        if len(sizes) > 1 and column == column_count - 1:
            sizes = sizes[:-1] + [128, 128]
        start = 0
        for size in sizes:
            units.append((column, start, size, (column * fs_rows + start) // 8))
            start += size
    if len(units) > 4:
        kinds = [LATE] * ALONG_FIRST + [MIDDLE] * (len(units) - ALONG_FIRST - ALONG_LAST) + [FINAL] * ALONG_LAST
    else:
        kinds = [MIDDLE] * len(units)
    return units, kinds


def span_of(units, kinds, wanted):
    chosen = [unit for unit, kind in zip(units, kinds) if kind in wanted]
    return slice(chosen[0][3], chosen[-1][3] + chosen[-1][2] // 8) if chosen else None


def kernel(
    fs_size, tp_size, units, kinds,
    normed_hbm, rec_cot_hbm, conv_hbm, gate_cot_hbm, rec_moment_hbm, rec_right_hbm, gate_moment_hbm, gate_left_hbm,
    gate_right_hbm,
    rec_new, gate_new, scales,
    normed, rec_cot, conv_out, gate_cot, rec_moment, rec_right, gate_moment, gate_left, gate_right,
    part, first, second, along, helped, grad, wide_along, wide_helped, thick_second,
    gate_part, gate_first, gate_second, gate_held, gate_along, gate_helped, gate_grad, gate_pre,
    sums, message, slots,
    in_sem, rec_send, kind_send, pair_recv, ring_recv, help_recv,
    gate_send, gate_recv, spread_recv, pre_send, pre_recv, cube_send, cube_recv, sum_send, sum_recv,
):
    fs, rep, tp = lax.axis_index("fs"), lax.axis_index("rep"), lax.axis_index("tp")
    bits = (lax.rem(rep, 2), rep // 2)
    partners = (rep + 1 - 2 * bits[0], rep + 2 - 4 * bits[1])
    width = part.shape[-1]
    fs_rows = rec_moment.shape[0]
    blocks = gate_moment.shape[0]
    masks = [2**i - 1 for i in range(1, fs_size.bit_length())]
    by_head = gate_pre is not None
    last = fs_size - 1
    gate = len(units)

    copies = []
    waits = {}

    def load(name, source, target, sem=None):
        sem = in_sem.at[len(waits)] if sem is None else sem
        copies.append(pltpu.make_async_copy(source, target, sem))
        waits.setdefault(name, (target, sem))
        return sem

    def column_of(k):
        return slice(units[k][0] * width, (units[k][0] + 1) * width)

    def fetch_columns(column):
        span = slice(column * width, (column + 1) * width)
        load(("cot", column), rec_cot_hbm.at[:, span], rec_cot.at[:, span])

    fetch_columns(0)
    for column, start, size, _ in units:
        if column == 0:
            sem = None
            for owner in range(fs_size):
                span = slice(owner * fs_rows + start, owner * fs_rows + start + size)
                sem = load(("normed", start), normed_hbm.at[:, span], normed.at[:, span], sem)
            waits["normed", start] = (normed.at[:, 0 : fs_size * size], sem)
            if start == 0:
                load("conv", conv_hbm, conv_out)
                load("gate", gate_cot_hbm, gate_cot)
    for column in range(1, units[-1][0] + 1):
        fetch_columns(column)
    load("right", rec_right_hbm, rec_right)
    load("moment", rec_moment_hbm, rec_moment)
    load("gate right", gate_right_hbm, gate_right)
    load("gate left", gate_left_hbm, gate_left)
    load("gate moment", gate_moment_hbm, gate_moment)
    for copy in copies:
        copy.start()

    def loaded(*names):
        for name in names:
            if name in waits:
                whole, sem = waits.pop(name)
                pltpu.make_async_copy(whole, whole, sem).wait()

    sizes = {"fs": fs_size, "rep": 4, "tp": tp_size}
    places = {"fs": fs, "rep": rep, "tp": tp}
    direct = fs_size * tp_size <= 8
    groups = [("fs", "tp"), ("rep",)] if direct else [("fs",), ("tp",), ("rep",)]
    counts = [math.prod(sizes[axis] for axis in axes) for axes in groups]

    def members(axes):
        return [
            {axis: lax.rem(places[axis] + move, sizes[axis]) for axis, move in zip(axes, moves)}
            for moves in itertools.product(*(range(sizes[axis]) for axis in axes))
            if any(moves)
        ]

    barrier = pltpu.get_barrier_semaphore()
    greeted = [peer for axes in groups for peer in members(axes)]
    for peer in greeted:
        pl.semaphore_signal(barrier, inc=1, device_id=peer, device_id_type=MESH)
    sums[...] = jnp.zeros_like(sums)

    def remote(source, target, send, recv, peer):
        return pltpu.make_async_remote_copy(
            src_ref=source, dst_ref=target, send_sem=send, recv_sem=recv,
            device_id=peer, device_id_type=MESH,
        )

    def arrived(whole, recv):
        remote(whole, whole, rec_send.at[0], recv, {"rep": partners[0]}).wait_recv()

    def sent(whole, send):
        remote(whole, whole, send, pair_recv.at[0, 0], {"rep": partners[0]}).wait_send()

    def mine(s):
        return bits[s], bits[1 - s]

    def rows_of(k):
        return slice(units[k][3], units[k][3] + units[k][2] // 8)

    def first_pair(k, s):
        a, _ = mine(s)
        here = rows_of(k)
        if kinds[k] == LATE:
            source, target, sem = part.at[s, 1 - a, :, fs, here], first.at[s, :, 0, here], kind_send.at[0]
        else:
            source, target, sem = part.at[s, 1 - a, :, :, here], first.at[s, :, :, here], rec_send.at[0]
        return remote(source, target, sem, pair_recv.at[k, 0], {"rep": partners[s]})

    def second_pair(k, s):
        a, b = mine(s)
        here = rows_of(k)
        if kinds[k] == FINAL:
            source, target, sem = part.at[s, a, 1 - b, :, here], thick_second.at[s, :, thick(k)], kind_send.at[1]
        else:
            source, target, sem = part.at[s, a, 1 - b, fs, here], second.at[s, here], rec_send.at[2]
        return remote(source, target, sem, pair_recv.at[k, 1], {"rep": partners[1 - s]})

    def gather_pair(k, s, level):
        a, b = mine(s)
        if level == 0:
            here = grad.at[s, a, b, rows_of(k)]
        else:
            here = grad.at[s, a, :, rows_of(k)]
        sem = kind_send.at[2 + level] if kinds[k] == FINAL else rec_send.at[2]
        return remote(here, here, sem, pair_recv.at[k, 2 + level], {"rep": partners[1 - s if level == 0 else s]})

    def thick(k):
        begin = units[k][3] - span_of(units, kinds, (FINAL,)).start
        return slice(begin, begin + units[k][2] // 8)

    def chunk(k, s, owner):
        a, b = mine(s)
        if k == gate:
            return gate_part.at[s, a, b, owner]
        if kinds[k] == LATE:
            return part.at[s, :, :, owner, rows_of(k)]
        return part.at[s, a, b if kinds[k] == FINAL else slice(None), owner, rows_of(k)]

    def ring_slots(k, s, steps):
        if k == gate:
            return gate_along.at[s, steps]
        if kinds[k] == LATE:
            return wide_along.at[s, steps, :, :, rows_of(k)]
        return along.at[s, steps, 0 if kinds[k] == FINAL else slice(None), rows_of(k)]

    def ring_slot(k, s, step):
        return ring_slots(k, s, step - 1)

    def help_slot(k, s):
        if k == gate:
            return gate_helped.at[s]
        if kinds[k] == LATE:
            return wide_helped.at[s, :, :, rows_of(k)]
        return helped.at[s, 0 if kinds[k] == FINAL else slice(None), rows_of(k)]

    def ring_sem(k):
        if k == gate:
            return gate_send.at[2]
        return rec_send.at[1] if kinds[k] == MIDDLE else kind_send.at[4 if kinds[k] == LATE else 5]

    def ring(k, s, step):
        peer = lax.rem(fs + step, fs_size)
        return remote(chunk(k, s, peer), ring_slot(k, s, step), ring_sem(k), ring_recv.at[k], {"fs": peer})

    def helper(k, s):
        return remote(
            chunk(k, s, last - fs), help_slot(k, s), ring_sem(k), help_recv.at[k],
            {"fs": jnp.where(fs == 0, 1, last - 1)},
        )

    at_end = (fs == 0) | (fs == last)
    beside = (fs == 1) | (fs == last - 1)
    fold_step = jnp.where(fs == 1, last - 1, 2)

    def when(condition, action):
        if condition is None:
            action()
        else:
            pl.when(condition)(action)

    def sends(step):
        skip = []
        if step == last:
            skip.append(fs == 0)
        if step == 1:
            skip.append(fs == last)
        if step == last - 1:
            skip.append(fs == 1)
        if step == 2:
            skip.append(fs == last - 1)
        return jnp.logical_not(functools.reduce(jnp.logical_or, skip)) if skip else None

    def receives(step):
        if step == last:
            return fs != last
        if step == 1:
            return fs != 0
        return None

    def ring_open(k, s):
        pl.when(at_end)(lambda: helper(k, s).start())
        for step in sorted(range(1, fs_size), key=lambda step: -min(step, fs_size - step)):
            when(sends(step), lambda step=step: ring(k, s, step).start())

    def fold(k):
        @pl.when(beside)
        def _():
            arrived(help_slot(k, slice(None)), help_recv.at[k])
            for s in range(2):
                whole = chunk(k, s, lax.rem(fs + fold_step, fs_size))
                whole[...] += help_slot(k, s)[...]
                ring(k, s, fold_step).start()

    def ring_close(k):
        def slots_of(count):
            return ring_slots(k, slice(None), slice(0, count))

        pl.when(at_end)(lambda: arrived(slots_of(last - 1), ring_recv.at[k]))
        pl.when(jnp.logical_not(at_end))(lambda: arrived(slots_of(last), ring_recv.at[k]))
        for s in range(2):
            own = chunk(k, s, fs)
            for step in range(1, fs_size):
                def take(own=own, s=s, step=step):
                    own[...] += ring_slot(k, s, step)[...]

                when(receives(step), take)

    def product(k):
        column, start, size, _ = units[k]
        loaded(("cot", column))
        loaded(("normed", start))

        @pl.loop(0, fs_size)
        def _(owner):
            begin = pl.multiple_of(owner * fs_rows + start, 128)
            term = token_dot(normed[:, pl.ds(begin, size)], rec_cot[:, column_of(k)])
            part[:, :, :, owner, rows_of(k)] = term.reshape(2, 2, 2, size // 8, width)

    def open_rec(k):
        product(k)
        if k == 0:
            pl.semaphore_wait(barrier, len(greeted))
        for s in range(2):
            if kinds[k] == LATE:
                ring_open(k, s)
            else:
                first_pair(k, s).start()

    def add_first(k, s):
        a, _ = mine(s)

        @pl.loop(0, fs_size)
        def _(owner):
            for b in range(2):
                part[s, a, b, owner, rows_of(k)] += first[s, b, owner, rows_of(k)]

    def spread(k):
        arrived(first.at[:, :, :, rows_of(k)], pair_recv.at[k, 0])
        for s in range(2):
            add_first(k, s)
            ring_open(k, s)

    def collect(k):
        ring_close(k)
        for s in range(2):
            second_pair(k, s).start()

    def collect_late(k):
        ring_close(k)
        for s in range(2):
            first_pair(k, s).start()

    def add_late(k):
        arrived(first.at[:, :, 0, rows_of(k)], pair_recv.at[k, 0])
        for s in range(2):
            a, _ = mine(s)
            part[s, a, :, fs, rows_of(k)] += first[s, :, 0, rows_of(k)]
            second_pair(k, s).start()

    def halve(k):
        arrived(first.at[:, :, :, rows_of(k)], pair_recv.at[k, 0])
        for s in range(2):
            add_first(k, s)
            second_pair(k, s).start()

    def spread_final(k):
        arrived(thick_second.at[:, :, thick(k)], pair_recv.at[k, 1])
        for s in range(2):
            a, b = mine(s)
            part[s, a, b, :, rows_of(k)] += thick_second[s, :, thick(k)]
            ring_open(k, s)

    def settle(k):
        loaded("right", "moment")
        if kinds[k] == FINAL:
            ring_close(k)
        else:
            arrived(second.at[:, rows_of(k)], pair_recv.at[k, 1])
        _, start, size, _ = units[k]
        rows = size // 8
        gradients, moments = [], []
        for s in range(2):
            a, b = mine(s)
            quarter = part[s, a, b, fs, rows_of(k)]
            gradients.append(quarter if kinds[k] == FINAL else quarter + second[s, rows_of(k)])
            begin = pl.multiple_of(start + (4 * s + 2 * a + b) * rows, 8)
            moments.append(rec_moment[pl.ds(begin, rows), column_of(k)])
        gradient = jnp.concatenate(gradients, axis=0)
        moment = BETA * jnp.concatenate(moments, axis=0) + split_dot(gradient, rec_right[column_of(k), :])
        for s in range(2):
            a, b = mine(s)
            grad[s, a, b, rows_of(k)] = moment[s * rows : (s + 1) * rows]
            gather_pair(k, s, 0).start()
        sums[0] += folded_squares(gradient)
        sums[1] += folded_squares(moment)

    def forward(k):
        arrived(grad.at[0, :, 0, rows_of(k)], pair_recv.at[k, 2])
        for s in range(2):
            gather_pair(k, s, 1).start()

    def finish(k):
        arrived(grad.at[0, :, :, rows_of(k)], pair_recv.at[k, 3])
        _, start, size, _ = units[k]
        rec_new[start : start + size, column_of(k)] = grad[:, :, :, rows_of(k)].reshape(size, width)

    def gate_pair(s, index):
        a, b = mine(s)
        source, target = (gate_part.at[s, 1 - a], gate_first) if index == 0 else (gate_part.at[s, a, 1 - b], gate_second)
        return remote(
            source, target.at[s], gate_send.at[index], gate_recv.at[index],
            {"rep": partners[s if index == 0 else 1 - s]},
        )

    def open_gate():
        loaded("conv", "gate")

        @pl.loop(0, blocks)
        def _(block):
            columns = pl.ds(pl.multiple_of(block * width, width), width)
            term = token_dot(conv_out[:, columns], gate_cot[:, columns])
            if by_head:
                each, thin = gate_part.shape[4], gate_part.shape[5]
                head, place = block // each, lax.rem(block, each)
                halves = term.reshape(2, fs_size, thin, width)
                gate_part[0, head // 2, lax.rem(head, 2), :, place] = halves[0]
                gate_part[1, lax.rem(head, 2), head // 2, :, place] = halves[1]
            else:
                gate_part[:, :, :, block] = term.reshape(2, 2, 2, gate_part.shape[4], width)

        for s in range(2):
            gate_pair(s, 0).start()

    def gate_add_first():
        arrived(gate_first, gate_recv.at[0])
        for s in range(2):
            a, _ = mine(s)
            gate_part[s, a] += gate_first[s]
            gate_pair(s, 1).start()

    def gate_total(s):
        if s == 0:
            arrived(gate_second, gate_recv.at[1])
        a, b = mine(s)
        return gate_part[s, a, b] + gate_second[s]

    def gate_scatter():
        for s in range(2):
            a, b = mine(s)
            gate_part[s, a, b] = gate_total(s)
            ring_open(gate, s)

    def broadcast(s, step):
        return remote(
            gate_grad.at[s, fs], gate_grad.at[s, fs], gate_send.at[3], spread_recv.at[0],
            {"fs": lax.rem(fs + step, fs_size)},
        )

    def gate_collect():
        ring_close(gate)
        for s in range(2):
            a, b = mine(s)
            gate_grad[s, fs] = gate_part[s, a, b, fs]
            for step in range(1, fs_size):
                broadcast(s, step).start()

    def pre_pair(level):
        here = gate_pre.at[bits[0], bits[1]] if level == 0 else gate_pre.at[bits[0]]
        return remote(here, here, pre_send.at[level], pre_recv.at[level], {"rep": partners[1 - level]})

    def gate_product():
        arrived(gate_along, spread_recv.at[0])
        loaded("gate right", "gate left", "gate moment")
        each = gate_part.shape[4]
        for place in range(each):
            block = (2 * bits[0] + bits[1]) * each + place
            gradient = gate_grad[:, :, place].reshape(width, width)
            right_done = split_dot(gradient, gate_right[block])
            moment = BETA * gate_moment[block] + split_dot_left(gate_left[block], right_done)
            gate_pre[bits[0], bits[1], place] = moment
            sums[2] += folded_squares(gradient) * (1.0 / fs_size)
            sums[3] += folded_squares(moment)
        pre_pair(0).start()

    def gate_forward():
        pre_pair(0).wait_recv()
        pre_pair(1).start()

    def gate_finish():
        pre_pair(1).wait_recv()
        each = gate_part.shape[4]
        for block in range(blocks):
            head, place = block // each, block % each
            gate_new[block] = gate_pre[head // 2, head % 2, place]

    def cube(s, step):
        mask = masks[step] if s == 0 else masks[-1 - step]
        return remote(
            gate_held.at[s, step], gate_along.at[s, step], cube_send.at[s, step], cube_recv.at[s, step],
            {"fs": fs ^ mask},
        )

    def whole_pair(s, level):
        a, b = mine(s)
        here = gate_grad.at[s, a, b] if level == 0 else gate_grad.at[s, a]
        return remote(
            here, here, pre_send.at[2 * s + level], pre_recv.at[2 * s + level],
            {"rep": partners[1 - s if level == 0 else s]},
        )

    def cube_open():
        for s in range(2):
            gate_held[s, 0] = gate_total(s)
            cube(s, 0).start()

    def cube_add(step):
        for s in range(2):
            cube(s, step).wait_recv()
            total = gate_held[s, step] + gate_along[s, step]
            if step + 1 < len(masks):
                gate_held[s, step + 1] = total
                cube(s, step + 1).start()
            else:
                a, b = mine(s)
                gate_grad[s, a, b] = total
                whole_pair(s, 0).start()

    def whole_forward():
        for s in range(2):
            whole_pair(s, 0).wait_recv()
            whole_pair(s, 1).start()

    def whole_finish():
        for s in range(2):
            whole_pair(s, 1).wait_recv()
        loaded("gate right", "gate left", "gate moment")

        @pl.loop(0, blocks)
        def _(block):
            gradient = gate_grad[:, :, :, block].reshape(width, width)
            right_done = split_dot(gradient, gate_right[block])
            moment = BETA * gate_moment[block] + split_dot_left(gate_left[block], right_done)
            gate_new[block] = moment
            sums[2] += folded_squares(gradient) * (0.25 / fs_size)
            sums[3] += folded_squares(moment) * 0.25

    def rec_stages(k):
        middle = {
            LATE: (fold, collect_late, add_late), MIDDLE: (spread, fold, collect), FINAL: (halve, spread_final, fold)
        }[kinds[k]]
        return [functools.partial(f, k) for f in (open_rec, *middle, settle, forward, finish)]

    gate_stages = [open_gate, gate_add_first]
    if by_head:
        gate_stages += [gate_scatter, functools.partial(fold, gate), gate_collect, gate_product, gate_forward, gate_finish]
    else:
        gate_stages += [cube_open, *(functools.partial(cube_add, step) for step in range(len(masks)))]
        gate_stages += [whole_forward, whole_finish]
    queue = [rec_stages(k) for k in range(len(units))]
    queue.insert(min(GATE_PLACE, len(queue)), gate_stages)

    agenda = []
    for place, stages in enumerate(queue):
        offsets = GATE_AT if stages is gate_stages else REC_AT
        for stage, action in enumerate(stages):
            offset = offsets[stage] if stage < len(offsets) else offsets[-1] + stage + 1 - len(offsets)
            tick = OPEN_AT[place] if stage == 0 and place < len(OPEN_AT) else max(0, place + offset)
            agenda.append((tick, stage > 0, -place if stage else place, stage, action))

    def exchange_open(index):
        axes, base = groups[index], sum(counts[:index])
        me = base
        scale = 1
        for axis in reversed(axes):
            me = me + places[axis] * scale
            scale *= sizes[axis]
        slots[me] = message[...]
        for peer in members(axes):
            remote(message, slots.at[me], sum_send.at[index], sum_recv.at[index], peer).start()

    def exchange_close(index):
        base = sum(counts[:index])
        others = slots.at[base : base + counts[index] - 1]
        arrived(others, sum_recv.at[index])
        sent(others, sum_send.at[index])
        message[...] = jnp.sum(slots[base : base + counts[index]], axis=0)

    adding = {settle, gate_product, whole_finish}
    left = sum(getattr(entry[-1], "func", entry[-1]) in adding for entry in agenda)
    for tick, _, place, stage, action in sorted(agenda, key=lambda entry: entry[:4]):
        action()
        if getattr(action, "func", action) in adding:
            left -= 1
            if not left:
                for i in range(4):
                    message[i : i + 1] = jnp.sum(sums[i], axis=0, keepdims=True)
                message[4:8] = jnp.zeros((4, LANES), jnp.float32)
                exchange_open(0)
        elif left == 0:
            exchange_close(0)
            exchange_open(1)
            left = None

    if left is not None:
        exchange_close(0)
        exchange_open(1)
    for index in range(1, len(groups)):
        exchange_close(index)
        if index + 1 < len(groups):
            exchange_open(index + 1)
    total = message[...]
    squares = [jnp.sum(total[i : i + 1], keepdims=True) for i in range(4)]
    rec_scale = jnp.sqrt(squares[0]) / jnp.sqrt(squares[1] + EPSILON)
    gate_scale = jnp.sqrt(squares[2]) / jnp.sqrt(squares[3] + EPSILON)
    scales[0] = jnp.broadcast_to(rec_scale, (8, LANES))
    scales[1] = jnp.broadcast_to(gate_scale, (8, LANES))

    early = span_of(units, kinds, (MIDDLE, FINAL))
    sent(first.at[:, :, :, early], rec_send.at[0])
    sent(along.at[:, :, :, span_of(units, kinds, (MIDDLE,))], rec_send.at[1])
    sent(grad.at[:, :, :, span_of(units, kinds, (LATE, MIDDLE))], rec_send.at[2])
    if LATE in kinds:
        sent(first.at[:, :, 0, span_of(units, kinds, (LATE,))], kind_send.at[0])
        sent(wide_along, kind_send.at[4])
    if FINAL in kinds:
        sent(thick_second, kind_send.at[1])
        final = span_of(units, kinds, (FINAL,))
        sent(grad.at[0, :, 0, final], kind_send.at[2])
        sent(grad.at[0, :, :, final], kind_send.at[3])
        sent(along.at[:, :, 0, final], kind_send.at[5])
    sent(gate_first, gate_send.at[0])
    sent(gate_second, gate_send.at[1])
    if by_head:
        sent(gate_along, gate_send.at[2])
        sent(gate_along, gate_send.at[3])
        for level in range(2):
            pre_pair(level).wait_send()
    else:
        for s in range(2):
            for step in range(len(masks)):
                cube(s, step).wait_send()
            for level in range(2):
                whole_pair(s, level).wait_send()


def update_kernel(
    rec_weight, gate_weight, rec_new, gate_new, scales,
    rec_weight_out, rec_new_out, rec_step_out, rec_copy_out,
    gate_weight_out, gate_new_out, gate_step_out, gate_copy_out,
    rec_after, rec_step, rec_copy, gate_after, gate_step, gate_copy,
    out_sem,
):
    groups = (
        (rec_weight, rec_new, rec_after, rec_step, rec_copy, rec_weight_out, rec_new_out, rec_step_out, rec_copy_out),
        (gate_weight, gate_new, gate_after, gate_step, gate_copy,
         gate_weight_out, gate_new_out, gate_step_out, gate_copy_out),
    )
    copies = []
    for group, (weight, new, after, step, copy, *outs) in enumerate(groups):
        parts = PARTS if weight.shape[0] % PARTS == 0 else 1
        size = weight.shape[0] // parts
        factor = LEARN_RATE * scales[group, 0:1, 0:1]
        for i in range(parts):
            here = slice(i * size, (i + 1) * size)
            moved = pltpu.make_async_copy(new.at[here], outs[1].at[here], out_sem.at[group, i, 1])
            moved.start()
            copies.append(moved)
        for i in range(parts):
            here = slice(i * size, (i + 1) * size)
            moment = new[here]
            taken = (factor if moment.ndim == 2 else factor[None]) * moment
            step[here] = taken
            result = weight[here] - taken
            after[here] = result
            copy[here] = result.astype(jnp.bfloat16)
            for index, source in ((0, after), (2, step), (3, copy)):
                moved = pltpu.make_async_copy(source.at[here], outs[index].at[here], out_sem.at[group, i, index])
                moved.start()
                copies.append(moved)
    for moved in copies:
        moved.wait()


def shards(fs_size, rep_size, tp_size, normed, rec_cot, conv_out, gate_cot, rec_weight, rec_moment,
           rec_right, gate_weight, gate_moment, gate_left, gate_right):
    assert rep_size == 4 and fs_size & (fs_size - 1) == 0 and fs_size >= 4
    f32 = jnp.float32
    fs_rows, columns = rec_weight.shape
    width = rec_right.shape[1]
    blocks, gate_rows = gate_weight.shape[:2]
    units, kinds = plan(fs_rows, columns // width)
    late_span, final_span = span_of(units, kinds, (LATE,)), span_of(units, kinds, (FINAL,))
    late, final = (span.stop - span.start if span else None for span in (late_span, final_span))
    rows = fs_rows * (columns // width) // 8
    others = fs_size - 1
    cubes = fs_size.bit_length() - 1
    groups, tiles = (2, fs_size * tp_size + rep_size) if fs_size * tp_size <= 8 else (3, fs_size + tp_size + rep_size)
    loads = columns // width + sum(unit[0] == 0 for unit in units) + 7
    operands = (normed, rec_cot, conv_out, gate_cot, rec_moment, rec_right, gate_moment, gate_left, gate_right)
    vmem = pl.BlockSpec(memory_space=pltpu.VMEM)
    dma = pltpu.SemaphoreType.DMA
    by_head = blocks % 4 == 0
    if by_head:
        thin = (blocks // 4, width // 2 // fs_size, width)
        piece = (fs_size, *thin)
        gate_held = None
        gate_along = pltpu.VMEM((2, others, *thin), f32)
        gate_helped = pltpu.VMEM((2, *thin), f32)
        gate_grad = pltpu.VMEM((2, *piece), f32)
        gate_pre = pltpu.VMEM((2, 2, blocks // 4, gate_rows, width), f32)
    else:
        piece = (blocks, width // 8, width)
        gate_held = pltpu.VMEM((2, cubes, *piece), f32)
        gate_along = pltpu.VMEM((2, cubes, *piece), f32)
        gate_helped = None
        gate_grad = pltpu.VMEM((2, 2, 2, *piece), f32)
        gate_pre = None
    rec_new, gate_new, scales = pl.pallas_call(
        functools.partial(kernel, fs_size, tp_size, units, kinds),
        out_shape=(
            pltpu.VMEM(rec_weight.shape, f32),
            pltpu.VMEM(gate_weight.shape, f32),
            pltpu.VMEM((2, 8, LANES), f32),
        ),
        in_specs=[pl.BlockSpec(memory_space=pltpu.HBM)] * len(operands),
        out_specs=(vmem,) * 3,
        scratch_shapes=[
            *(pltpu.VMEM(x.shape, x.dtype) for x in operands),
            pltpu.VMEM((2, 2, 2, fs_size, rows, width), f32),
            pltpu.VMEM((2, 2, fs_size, rows, width), f32),
            pltpu.VMEM((2, rows, width), f32),
            pltpu.VMEM((2, others, 2, rows, width), f32),
            pltpu.VMEM((2, 2, rows, width), f32),
            pltpu.VMEM((2, 2, 2, rows, width), f32),
            late and pltpu.VMEM((2, others, 2, 2, late, width), f32),
            late and pltpu.VMEM((2, 2, 2, late, width), f32),
            final and pltpu.VMEM((2, fs_size, final, width), f32),
            pltpu.VMEM((2, 2, 2, *piece), f32),
            pltpu.VMEM((2, 2, *piece), f32),
            pltpu.VMEM((2, *piece), f32),
            gate_held,
            gate_along,
            gate_helped,
            gate_grad,
            gate_pre,
            pltpu.VMEM((4, 8, LANES), f32),
            pltpu.VMEM((8, LANES), f32),
            pltpu.VMEM((tiles, 8, LANES), f32),
            dma((loads,)),
            dma((3,)),
            dma((6,)),
            dma((len(units), 4)),
            dma((len(units) + 1,)),
            dma((len(units) + 1,)),
            dma((4,)),
            dma((2,)),
            dma((1,)),
            dma((4,)),
            dma((4,)),
            None if by_head else dma((2, cubes)),
            None if by_head else dma((2, cubes)),
            dma((groups,)),
            dma((groups,)),
        ],
        compiler_params=pltpu.CompilerParams(
            collective_id=0, has_side_effects=True, vmem_limit_bytes=44 * 1024 * 1024
        ),
    )(*(pltpu.with_memory_space_constraint(x, pltpu.HBM) for x in operands))

    return update(rec_weight, gate_weight, rec_new, gate_new, scales)


def update(rec_weight, gate_weight, rec_new, gate_new, scales):
    vmem = pl.BlockSpec(memory_space=pltpu.VMEM)
    hbm = pl.BlockSpec(memory_space=pltpu.HBM)
    f32, bf16 = jnp.float32, jnp.bfloat16
    weights = (rec_weight, gate_weight)
    shapes = [jax.ShapeDtypeStruct(w.shape, t) for w in weights for t in (f32, f32, f32, bf16)]
    return pl.pallas_call(
        update_kernel,
        out_shape=shapes,
        in_specs=[vmem] * 5,
        out_specs=[hbm] * 8,
        scratch_shapes=[
            *(pltpu.VMEM(w.shape, t) for w in weights for t in (f32, f32, bf16)),
            pltpu.SemaphoreType.DMA((2, PARTS, 4)),
        ],
        compiler_params=pltpu.CompilerParams(vmem_limit_bytes=16 * 1024 * 1024),
    )(
        *(pltpu.with_memory_space_constraint(x, pltpu.VMEM) for x in (rec_weight, gate_weight, rec_new, gate_new, scales))
    )


def solution(mesh):
    in_specs = (
        P(("fs", "rep"), None),
        P(("fs", "rep"), "tp"),
        P(("fs", "rep"), "tp"),
        P(("fs", "rep"), "tp"),
        P("fs", "tp"),
        P("fs", "tp"),
        P("tp", None),
        P("tp", "fs", None),
        P("tp", "fs", None),
        P("tp", "fs", None),
        P("tp", None, None),
    )
    out_specs = (P("fs", "tp"),) * 4 + (P("tp", "fs", None),) * 4
    body = functools.partial(shards, mesh.shape["fs"], mesh.shape["rep"], mesh.shape["tp"])
    return jax.shard_map(body, mesh=mesh, in_specs=in_specs, out_specs=out_specs, check_vma=False)
```
